32 devices in a mesh: rep: 2 (over y), fs: 4 (over z), tp: 4 (over x, core).
Axes of the slice: x: 2, y: 2, z: 4, core: 2. Of those that a mesh axis runs over, the one named last changes fastest.
Arguments:
- tokens: bfloat16 [2048, 2048], P(('rep', 'fs')), may hold values from -6 to 6
- norm_gains: float32 [3, 2048], replicated, may hold values from 0.1 to 1.9
- gate_weight: float32 [2048, 3072], P('fs', 'tp'), may hold values from -0.125 to 0.125
- up_weight: float32 [2048, 3072], P('fs', 'tp'), may hold values from -0.125 to 0.125
- hidden_scales: float32 [2, 3072], P(None, 'tp'), may hold values from 0.5 to 2
- down_weight: float32 [3072, 2048], P('tp', 'fs'), may hold values from -0.21875 to 0.21875
- down_scale: float32 [2048], P('fs'), may hold values from 0.5 to 2
- mix_in: float32 [2048, 512], P('fs'), may hold values from -0.125 to 0.125
- in_scale: float32 [512], replicated, may hold values from 0.5 to 2
- pool_map: float32 [4, 128, 128], replicated, may hold values from -0.5 to 0.5
- pool_scale: float32 [512], P('tp'), may hold values from 0.5 to 2
- mix_out: float32 [512, 2048], P('tp', 'fs'), may hold values from -0.25 to 0.25
- out_scale: float32 [2048], P('fs'), may hold values from 0.5 to 2
Outputs:
- layer_out: bfloat16 [2048, 2048], P(('rep', 'fs'))
The draws below stay inside these ranges and needn't reach their ends.
All inputs are finite; a program needn't handle non-finite values.
Results may differ from the reference program's by a relative error of at most 0.02.
Values may be sent and summed in bfloat16 or wider, within the bound.
A program may use at most 64 MiB of HBM per device.

```python
import math
import jax
import jax.numpy as jnp
from jax import lax

D = 2048
FF = 3072
DP = 512
GROUPS = 4
GC = 128
TOK = 256
TOKENS = 2048
N_TP = 4


def steps_of(key, shape, pieces, least, largest):
    factor_of, own = 1.0, jax.random.fold_in(key, 6)
    for axis_at, shards_of in pieces:
        heights = jnp.exp(jax.random.uniform(jax.random.fold_in(own, axis_at), (shards_of,), jnp.float32, least / len(pieces), largest / len(pieces)))
        factor_of = factor_of * jnp.repeat(heights, shape[axis_at] // shards_of).reshape([-1 if axis == axis_at else 1 for axis in range(len(shape))])
    return factor_of


def centred(key, shape, spread, bound, cuts=(), kind=jnp.bfloat16):
    entries = jax.random.normal(key, shape, jnp.float32) * spread
    if len(cuts) > 0:
        entries = steps_of(key, shape, cuts, -0.22, 0.18) * entries
    return jnp.clip(entries, min=-bound, max=bound).astype(kind)


def setup_inputs(seed: int = 0) -> dict:
    keys = jax.random.split(jax.random.key(seed), 14)
    tokens = centred(keys[0], (TOKENS, D), 1.0, 6.0, ((0, 8),))
    norm_gains = jnp.clip(1.0 + 0.18 * jax.random.normal(keys[1], (3, D), jnp.float32), 0.1, 1.9)
    gate_weight = centred(keys[2], (D, FF), D ** -0.5, 0.125, ((0, 4), (1, 4)), jnp.float32)
    up_weight = centred(keys[3], (D, FF), D ** -0.5, 0.125, ((0, 4), (1, 4)), jnp.float32)
    hidden_scales = jnp.clip(jnp.exp(math.log(2.0) - 1.3862944 * jax.random.uniform(keys[4], (2, FF), jnp.float32) ** steps_of(keys[4], (2, FF), ((1, 4),), -0.2, 0.2)), 0.5, 2.0)
    down_weight = centred(keys[5], (FF, D), (FF // 4) ** -0.5, 0.21875, ((0, 4), (1, 4)), jnp.float32)
    down_scale = jnp.clip(jnp.exp(math.log(2.0) - 1.3862944 * jax.random.uniform(keys[6], (D,), jnp.float32) ** steps_of(keys[6], (D,), ((0, 4),), -0.2, 0.2)), 0.5, 2.0)
    mix_in = centred(keys[7], (D, DP), D ** -0.5, 0.125, ((0, 4),), jnp.float32)
    in_scale = jnp.clip(jnp.exp(jax.random.uniform(keys[8], (DP,), jnp.float32, math.log(0.5), math.log(2.0))), 0.5, 2.0)
    pool_map = centred(keys[9], (GROUPS, GC, GC), GC ** -0.5, 0.5, (), jnp.float32)
    pool_scale = jnp.clip(jnp.exp(math.log(2.0) - 1.3862944 * jax.random.uniform(keys[10], (DP,), jnp.float32) ** steps_of(keys[10], (DP,), ((0, 4),), -0.2, 0.2)), 0.5, 2.0)
    mix_out = centred(keys[11], (DP, D), DP ** -0.5, 0.25, ((0, 4), (1, 4)), jnp.float32)
    out_scale = jnp.clip(jnp.exp(math.log(2.0) - 1.3862944 * jax.random.uniform(keys[12], (D,), jnp.float32) ** steps_of(keys[12], (D,), ((0, 4),), -0.2, 0.2)), 0.5, 2.0)
    return {"tokens": tokens, "norm_gains": norm_gains, "gate_weight": gate_weight, "up_weight": up_weight, "hidden_scales": hidden_scales, "down_weight": down_weight, "down_scale": down_scale, "mix_in": mix_in, "in_scale": in_scale, "pool_map": pool_map, "pool_scale": pool_scale, "mix_out": mix_out, "out_scale": out_scale}


eps = 1e-06
widest = 16

def normed(values, gain):
    mean_sq = lax.optimization_barrier(jnp.mean(values * values, axis=-1, keepdims=True))
    return (values * lax.rsqrt(mean_sq + eps) * gain).astype(jnp.bfloat16)

def feed_forward(hidden_in, gate_bf, up_bf, down_bf, hidden_scales, down_scale):
    gate = jnp.dot(hidden_in, gate_bf, preferred_element_type=jnp.float32) * hidden_scales[0]
    upper = jnp.dot(hidden_in, up_bf, preferred_element_type=jnp.float32) * hidden_scales[1]
    hidden = (jax.nn.silu(gate) * upper).astype(jnp.bfloat16)
    block_ff = FF // N_TP
    total = jnp.zeros((hidden_in.shape[0], D), jnp.float32)
    for block_index in range(N_TP):
        lower = block_index * block_ff
        part = jnp.dot(hidden[:, lower:lower + block_ff], down_bf[lower:lower + block_ff], preferred_element_type=jnp.float32)
        total = total + part.astype(jnp.bfloat16).astype(jnp.float32)
    return total * down_scale

def pool_rows(pool_in):
    values = pool_in.astype(jnp.float32)
    length = values.shape[1]
    channel = jnp.arange(DP, dtype=jnp.int32)
    window = jnp.left_shift(jnp.int32(2), channel // GC)
    position = jnp.arange(length, dtype=jnp.int32)[:, None]
    summed = jnp.zeros_like(values)
    for offset in range(widest):
        shifted = jnp.pad(values, ((0, 0), (offset, 0), (0, 0)))[:, :length]
        summed = summed + jnp.where(offset < window, shifted, 0.0)
    counts = jnp.minimum(position + 1, window).astype(jnp.float32)
    return (summed / counts - values).astype(jnp.bfloat16)

def reference(tokens, norm_gains, gate_weight, up_weight, hidden_scales, down_weight, down_scale, mix_in, in_scale, pool_map, pool_scale, mix_out, out_scale):
    gate_bf = gate_weight.astype(jnp.bfloat16)
    up_bf = up_weight.astype(jnp.bfloat16)
    down_bf = down_weight.astype(jnp.bfloat16)
    resid = tokens.astype(jnp.float32)
    first = normed(resid, norm_gains[0])
    resid_one = resid + 0.5 * feed_forward(first, gate_bf, up_bf, down_bf, hidden_scales, down_scale)
    second = normed(resid_one, norm_gains[1])
    pool_in = (jnp.dot(second, mix_in.astype(jnp.bfloat16), preferred_element_type=jnp.float32) * in_scale).astype(jnp.bfloat16)
    pooled = pool_rows(pool_in.reshape(-1, TOK, DP)).reshape(-1, GROUPS, GC)
    map_bf = pool_map.astype(jnp.bfloat16)
    grouped = jnp.einsum('rgc,gcd->rgd', pooled.astype(jnp.float32), map_bf.astype(jnp.float32))
    pool_out = (grouped.reshape(-1, DP) * pool_scale).astype(jnp.bfloat16)
    out_bf = mix_out.astype(jnp.bfloat16)
    block_dp = DP // N_TP
    mixed = jnp.zeros_like(resid)
    for block_index in range(N_TP):
        lower = block_index * block_dp
        part = jnp.dot(pool_out[:, lower:lower + block_dp], out_bf[lower:lower + block_dp], preferred_element_type=jnp.float32)
        mixed = mixed + part.astype(jnp.bfloat16).astype(jnp.float32)
    resid_two = resid_one + mixed * out_scale
    third = normed(resid_two, norm_gains[2])
    final = resid_two + 0.5 * feed_forward(third, gate_bf, up_bf, down_bf, hidden_scales, down_scale)
    return final.astype(jnp.bfloat16)
```

```python
import functools

import jax
import jax.numpy as jnp
from jax import lax
from jax.experimental import pallas as pl
from jax.experimental.pallas import tpu as pltpu
from jax.sharding import PartitionSpec as P

eps = 1e-06
widest = 16


def normed(values, gain):
    mean_sq = jnp.mean(values * values, axis=-1, keepdims=True)
    return (values * lax.rsqrt(mean_sq + eps) * gain).astype(jnp.bfloat16)


def scatter_rows(term_fn, share):
    return lax.psum_scatter(
        term_fn(jnp.int32(0), lax.axis_size("tp") * share).astype(jnp.bfloat16),
        "tp",
        scatter_dimension=0,
        tiled=True,
    ).astype(jnp.float32)


def whole_rows(values):
    return lax.all_gather(values, "tp", axis=0, tiled=True)


def fetch_mixer(in_cols, mix_out):
    return (
        lax.all_gather(in_cols.astype(jnp.bfloat16), "fs", axis=0, tiled=True),
        lax.all_gather(mix_out.astype(jnp.bfloat16), "fs", axis=1, tiled=True),
    )


def hidden_units(rows_in, gate_full, up_full, hidden_scales):
    gate = jnp.dot(rows_in, gate_full, preferred_element_type=jnp.float32) * hidden_scales[0]
    upper = jnp.dot(rows_in, up_full, preferred_element_type=jnp.float32) * hidden_scales[1]
    return (jax.nn.silu(gate) * upper).astype(jnp.bfloat16)


def ffn_partial(normed_rows, gate_full, up_full, down_full, hidden_scales, share):

    def term_rows(row_start, row_count):
        hidden = hidden_units(normed_rows, gate_full, up_full, hidden_scales)
        return jnp.dot(hidden, down_full, preferred_element_type=jnp.float32)

    return scatter_rows(term_rows, share)


def per_device(
    tokens,
    norm_gains,
    gate_weight,
    up_weight,
    hidden_scales,
    down_weight,
    down_scale,
    mix_in,
    in_scale,
    pool_map,
    pool_scale,
    mix_out,
    out_scale,
):
    tp_width = lax.axis_size("tp")
    tp_rank = lax.axis_index("tp")
    seq_rows = tokens.shape[0]
    share = seq_rows // tp_width
    local_channels = mix_out.shape[0]
    group_width = pool_map.shape[1]
    needed = max(group_width, local_channels)
    first_channel = tp_rank * local_channels
    in_start = first_channel // group_width * group_width
    in_cols = lax.dynamic_slice_in_dim(mix_in, in_start, needed, 1)
    scale_cols = lax.dynamic_slice_in_dim(in_scale, in_start, needed, 0)
    down_cols, out_cols = (
        lax.all_gather(down_scale, "fs", axis=0, tiled=True),
        lax.all_gather(out_scale, "fs", axis=0, tiled=True),
    )
    gate_bf = gate_weight.astype(jnp.bfloat16)
    up_bf = up_weight.astype(jnp.bfloat16)
    down_bf = down_weight.astype(jnp.bfloat16)
    resid_all = tokens.astype(jnp.float32)
    first = normed(resid_all, norm_gains[0])
    gate_full, up_full, down_full = (
        lax.all_gather(gate_bf, "fs", axis=0, tiled=True),
        lax.all_gather(up_bf, "fs", axis=0, tiled=True),
        lax.all_gather(down_bf, "fs", axis=1, tiled=True),
    )
    ffn_one = ffn_partial(first, gate_full, up_full, down_full, hidden_scales, share)
    own_rows = lax.dynamic_slice_in_dim(resid_all, tp_rank * share, share, 0)
    resid_one = own_rows + 0.5 * (ffn_one * down_cols)
    second = whole_rows(normed(resid_one, norm_gains[1]))
    in_full, out_full = fetch_mixer(in_cols, mix_out)
    pool_in = (jnp.dot(second, in_full, preferred_element_type=jnp.float32) * scale_cols).astype(
        jnp.bfloat16
    )
    channel = in_start + jnp.arange(needed, dtype=jnp.int32)
    window = jnp.left_shift(jnp.int32(2), channel // group_width)
    position = jnp.arange(seq_rows, dtype=jnp.int32)[:, None]
    values = pool_in.astype(jnp.float32)
    summed = jnp.zeros_like(values)
    for offset in range(widest):
        shifted = jnp.pad(values, ((offset, 0), (0, 0)))[:seq_rows]
        summed = summed + jnp.where(offset < window, shifted, 0.0)
    counts = jnp.minimum(position + 1, window).astype(jnp.float32)
    pooled = (summed / counts - values).astype(jnp.bfloat16)
    map_bf = pool_map.astype(jnp.bfloat16)
    if local_channels < group_width:
        group_index = first_channel // group_width
        column_start = first_channel % group_width
        map_cols = lax.dynamic_slice(
            map_bf, (group_index, jnp.int32(0), column_start), (1, group_width, local_channels)
        )[0]
        grouped = jnp.dot(pooled, map_cols, preferred_element_type=jnp.float32)
    else:
        held_groups = local_channels // group_width
        maps_held = lax.dynamic_slice_in_dim(map_bf, first_channel // group_width, held_groups, 0)
        grouped = jnp.einsum(
            "tgc,gcd->tgd",
            pooled.reshape(seq_rows, held_groups, group_width),
            maps_held,
            preferred_element_type=jnp.float32,
        ).reshape(seq_rows, local_channels)
    pool_out = (grouped * pool_scale).astype(jnp.bfloat16)

    def mixer_rows(row_start, row_count):
        return jnp.dot(pool_out, out_full, preferred_element_type=jnp.float32)

    mixed = scatter_rows(mixer_rows, share)
    resid_two = resid_one + mixed * out_cols
    third = whole_rows(normed(resid_two, norm_gains[2]))
    ffn_two = ffn_partial(third, gate_full, up_full, down_full, hidden_scales, share)
    final_rows = (resid_two + 0.5 * (ffn_two * down_cols)).astype(jnp.bfloat16)
    return whole_rows(final_rows)


MESH = pl.DeviceIdType.MESH
PARTS = (1, 1, 4, 4)
FIRST_PART = (0, 1, 2, 6, 10)
TILE = 256
CHUNKS = 2
MIXER_AFTER = 1
bf16 = jnp.bfloat16
f32 = jnp.float32


def fits_kernel(mesh):
    return mesh.shape["rep"] == 2 and mesh.shape["fs"] == 4 and mesh.shape["tp"] == 4


def layer_kernel(
    n, tok, gains, gate_hbm, up_hbm, hs, down_hbm, mix_in_hbm, mix_out_hbm, isc, pmap, pool_scale, down_scale, out_scale,
    out, wide_gate, wide_up, wide_down, wide_in, wide_out, sc_in, gu_own, dn_own, gu_buf, dn_buf, wi_all, wo_all, sc_all, ps_all,
    ptok, first, gacc, hidden, stage, rs_a, s_z, rs_z, s_x, rs_x, r1, second, pool, r2, third, ra_2, sz_2, rz_2, sx_2, rx_2,
    z_send, y_send, w_recv, sc_send, sc_recv, tp_send, tp_recv, tk_send, tk_recv, rs_send, rs_recv, ag_send, ag_recv, loc,
):
    rep, fs, me = lax.axis_index("rep"), lax.axis_index("fs"), lax.axis_index("tp")
    seq, width = tok.shape
    slab = width // n
    share = seq // 4
    rows_half = seq // 2
    halo = widest
    window = rows_half + halo
    units = hs.shape[1]
    hu = units // 2
    groups, gc = pmap.shape[0], pmap.shape[1]
    core, chip = me % 2, me // 2
    mate = me + 1 - 2 * core
    across = (me + 2) % 4
    diag = (mate + 2) % 4
    peers = {1: mate, 2: across, 3: diag}
    partner = fs + 1 - 2 * (fs % 2)
    far_mid = jnp.where(fs < 2, 2, 1)
    far_end = jnp.where(fs < 2, 3, 0)
    order = (fs, partner, far_mid, far_end)
    middle = (fs == 1) | (fs == 2)
    kind = jnp.where(middle, 1, 0)
    kind_of = (kind, 1 - kind, 1, 0)

    def owner_cols(i):
        return pl.ds(pl.multiple_of(order[i] * slab, slab), slab)

    def cols_of(rank):
        return pl.ds(pl.multiple_of(rank * gc, gc), gc)

    half = slab // 2
    mine_half = pl.ds(pl.multiple_of(rep * half, half), half)
    other_half = pl.ds(pl.multiple_of((1 - rep) * half, half), half)
    loads = [
        pltpu.make_async_copy(mix_in_hbm.at[:, cols_of(me)], wide_in, loc.at[0]),
        pltpu.make_async_copy(mix_out_hbm, wide_out, loc.at[1]),
        pltpu.make_async_copy(gate_hbm.at[mine_half, :], wide_gate.at[mine_half, :], loc.at[2]),
        pltpu.make_async_copy(up_hbm.at[mine_half, :], wide_up.at[mine_half, :], loc.at[3]),
        pltpu.make_async_copy(gate_hbm.at[other_half, :], wide_gate.at[other_half, :], loc.at[4]),
        pltpu.make_async_copy(up_hbm.at[other_half, :], wide_up.at[other_half, :], loc.at[5]),
        pltpu.make_async_copy(down_hbm, wide_down, loc.at[6]),
    ]
    for load in loads:
        load.start()
    barrier = pltpu.get_barrier_semaphore()
    for i in (1, 2, 3):
        pl.semaphore_signal(barrier, inc=1, device_id={"fs": order[i]}, device_id_type=MESH)
    for k in (1, 2, 3):
        pl.semaphore_signal(barrier, inc=1, device_id={"tp": peers[k]}, device_id_type=MESH)
    pl.semaphore_signal(barrier, inc=1, device_id={"rep": 1 - rep}, device_id_type=MESH)

    sc_in[...] = jnp.zeros_like(sc_in)
    sc_in[0:1, :] = down_scale[...]
    sc_in[1:2, :] = out_scale[...]
    ps_all[me] = jnp.broadcast_to(pool_scale[...], ps_all.shape[1:])

    WI, WO, GU, DN = range(4)

    def piece(t, i, at, own_kind=None):
        shard = order[i]
        if t == WI:
            return wi_all.at[shard, pl.ds(pl.multiple_of(at * half, half), half), cols_of(me)]
        if t == WO:
            rows = gc // 2
            return wo_all.at[shard, pl.ds(pl.multiple_of(me * gc + at * rows, rows), rows), :]
        ref = (gu_own if t == GU else dn_own).at[own_kind] if own_kind is not None else (gu_buf if t == GU else dn_buf).at[shard]
        rows = ref.shape[0] // (2 * PARTS[t])
        return ref.at[pl.ds(pl.multiple_of(at * rows, rows), rows), :]

    started = []

    def start_if(cond, copy):
        if cond is None:
            copy.start()
        else:
            @pl.when(cond)
            def _():
                copy.start()
        started.append((cond, copy))

    def wait_sent():
        for cond, copy in started:
            if cond is None:
                copy.wait_send()
            else:
                @pl.when(cond)
                def _():
                    copy.wait_send()
        started.clear()

    def remote(src, dst, s_sem, r_sem, dev, cond=None):
        start_if(cond, pltpu.make_async_remote_copy(
            src_ref=src, dst_ref=dst, send_sem=s_sem, recv_sem=r_sem, device_id=dev, device_id_type=MESH
        ))

    def landed(dst, s_sem, r_sem):
        pltpu.make_async_remote_copy(
            src_ref=dst, dst_ref=dst, send_sem=s_sem, recv_sem=r_sem, device_id={"tp": mate}, device_id_type=MESH
        ).wait_recv()

    def send_own(t, i, u, cond=None):
        at = rep * PARTS[t] + u
        remote(
            piece(t, 0, at, kind_of[i] if t >= GU else None), piece(t, 0, at),
            z_send.at[i - 1, FIRST_PART[t] + u], w_recv.at[fs, 2 * FIRST_PART[t] + at], {"fs": order[i]}, cond,
        )

    def arrived(t, i, at):
        landed(piece(t, i, at), z_send.at[0, 0], w_recv.at[order[i], 2 * FIRST_PART[t] + at])

    def relay(t, i, u):
        at = rep * PARTS[t] + u
        arrived(t, i, at)
        here = piece(t, i, at)
        sem = w_recv.at[order[i], 2 * FIRST_PART[t] + at]
        if t < GU and i > 1:
            remote(here, here, y_send.at[0, i, FIRST_PART[t] + u], sem, {"fs": partner}, middle)
        remote(here, here, y_send.at[1, i, FIRST_PART[t] + u], sem, {"rep": 1 - rep})

    def rest(t, i):
        for u in range(PARTS[t]):
            arrived(t, i, (1 - rep) * PARTS[t] + u)

    loads[0].wait()
    loads[1].wait()
    wi_all[fs, :, cols_of(me)] = wide_in[...].astype(bf16)
    wo_all[fs, pl.ds(pl.multiple_of(me * gc, gc), gc), :] = wide_out[...].astype(bf16)

    def cast_gate_up(start, count, kinds):
        @pl.loop(0, count // 32)
        def _(j):
            rows = pl.ds(pl.multiple_of(start + j * 32, 32), 32)
            for h in kinds:
                cols = pl.ds(h * hu if isinstance(h, int) else pl.multiple_of(h * hu, 128), hu)
                gu_own[h, rows, 0:hu] = wide_gate[rows, cols].astype(bf16)
                gu_own[h, rows, hu:] = wide_up[rows, cols].astype(bf16)

    def my_rows(rank):
        return pl.ds(pl.multiple_of(rank * share, share), share)

    pl.semaphore_wait(barrier, n - 1 + 4)
    remote(tok.at[my_rows(me), :], ptok.at[my_rows(me), :], tk_send.at[0], tk_recv.at[0], {"fs": partner})
    loads[2].wait()
    loads[3].wait()
    for u in range(PARTS[GU]):
        cast_gate_up(rep * half + u * (half // PARTS[GU]), half // PARTS[GU], (0, 1))
        for i in (3, 2, 1):
            send_own(GU, i, u)
        if u == MIXER_AFTER:
            for t in (WI, WO):
                for i in (2, 1):
                    send_own(t, i, 0)

    def spread(t, i, rank):
        return wi_all.at[order[i], :, cols_of(rank)] if t == WI else wo_all.at[order[i], pl.ds(pl.multiple_of(rank * gc, gc), gc), :]

    def share_mixer(i):
        for t in (WI, WO):
            mine = spread(t, i, me)
            remote(mine, mine, tp_send.at[t, i, 1], tp_recv.at[t, i, 1], {"tp": across})
            remote(mine, mine, tp_send.at[t, i, 0], tp_recv.at[t, i, 0], {"tp": mate})

    def pass_mixer(i):
        for t in (WI, WO):
            theirs = spread(t, i, across)
            landed(theirs, tp_send.at[t, i, 1], tp_recv.at[t, i, 1])
            remote(theirs, theirs, tp_send.at[t, i, 2], tp_recv.at[t, i, 2], {"tp": mate})

    def have_mixer(i):
        for t in (WI, WO):
            landed(spread(t, i, mate), tp_send.at[t, i, 0], tp_recv.at[t, i, 0])
            landed(spread(t, i, diag), tp_send.at[t, i, 2], tp_recv.at[t, i, 2])

    share_mixer(0)
    loads[4].wait()
    loads[5].wait()
    cast_gate_up((1 - rep) * half, half, (kind,))
    loads[6].wait()

    @pl.loop(0, hu // 32)
    def _(j):
        rows = pl.ds(pl.multiple_of(j * 32, 32), 32)
        for h in (0, 1):
            dn_own[h, rows, :] = wide_down[pl.ds(pl.multiple_of(h * hu + j * 32, 32), 32), :].astype(bf16)

    for i in (1, 2, 3):
        remote(sc_in, sc_all.at[fs], sc_send.at[i - 1], sc_recv.at[fs], {"fs": order[i]})
    for k in (1, 2, 3):
        remote(ps_all.at[me], ps_all.at[me], tp_send.at[2, 0, k - 1], tp_recv.at[2, 0, k - 1], {"tp": peers[k]})

    def normed_rows(values, gain):
        mean_sq = jnp.mean(values * values, axis=-1, keepdims=True)
        return (values * lax.rsqrt(mean_sq + eps) * gain).astype(bf16)

    stage[:, :, 0:halo, :] = jnp.zeros((n, 2, halo, slab), bf16)

    def norm_first(source, top):
        @pl.loop(0, seq // 32)
        def _(j):
            rows = pl.ds(pl.multiple_of(j * 32, 32), 32)
            first[pl.ds(pl.multiple_of(top + j * 32, 32), 32), :] = normed_rows(source[rows, :].astype(f32), gains[0:1, :])

    def dot(a, b):
        return jnp.dot(a, b, preferred_element_type=f32)

    def held_gu(i):
        return gu_own.at[kind] if i == 0 else gu_buf.at[order[i]]

    def held_dn(i):
        return dn_own.at[kind] if i == 0 else dn_buf.at[order[i]]

    def gate_up(i, fresh):
        weights = held_gu(i)
        cols = owner_cols(i)

        @pl.loop(0, 2 * hu // TILE)
        def _(j):
            at = pl.ds(pl.multiple_of(j * TILE, TILE), TILE)
            term = dot(first[:, cols], weights[:, at])
            if fresh:
                gacc[:, at] = term
            else:
                gacc[:, at] += term

    def activate(rows):
        @pl.loop(0, hu // 128)
        def _(j):
            at = pl.ds(pl.multiple_of(j * 128, 128), 128)
            up_at = pl.ds(pl.multiple_of(hu + j * 128, 128), 128)
            sc_at = pl.ds(pl.multiple_of(kind * hu + j * 128, 128), 128)
            gate = gacc[rows, at] * hs[0:1, sc_at]
            upper = gacc[rows, up_at] * hs[1:2, sc_at]
            hidden[rows, at] = (gate / (1.0 + jnp.exp(-gate)) * upper).astype(bf16)

    def down(i, side, top):
        weights = held_dn(i)

        @pl.loop(0, slab // TILE)
        def _(j):
            at = pl.ds(pl.multiple_of(j * TILE, TILE), TILE)
            stage[i, side, top:top + seq, at] = dot(hidden[side * seq:(side + 1) * seq, :], weights[:, at]).astype(bf16)

    norm_first(tok, 0)
    own_rows = my_rows(me)
    landed(ptok.at[own_rows, :], tk_send.at[0], tk_recv.at[0])
    for k in (2, 3, 1):
        remote(ptok.at[own_rows, :], ptok.at[own_rows, :], tk_send.at[k], tk_recv.at[k], {"tp": peers[k]})
    def relay_mixer(i):
        for t in (WI, WO):
            relay(t, i, 0)

    def rest_mixer(i):
        rest(WI, i)
        rest(WO, i)
        share_mixer(i)

    for u in range(PARTS[GU]):
        for i in (1, 2, 3):
            relay(GU, i, u)
        if u == 1:
            for k in (1, 2, 3):
                landed(ptok.at[my_rows(peers[k]), :], tk_send.at[k], tk_recv.at[k])
            norm_first(ptok, seq)
        if u == 2:
            relay_mixer(1)
            for i in (1, 2, 3):
                for v in range(PARTS[DN]):
                    send_own(DN, i, v, middle if i == 3 else None)
            gate_up(0, True)
    relay_mixer(2)
    relay_mixer(3)
    rest_mixer(1)
    rest(GU, 1)
    gate_up(1, False)
    pass_mixer(0)
    rest(GU, 2)
    gate_up(2, False)
    rest_mixer(2)
    rest_mixer(3)
    rest(GU, 3)
    gate_up(3, False)
    activate(slice(None))

    for i in (1, 2, 3):
        landed(sc_all.at[order[i]], sc_send.at[0], sc_recv.at[order[i]])

    def scales(i):
        return sc_in if i == 0 else sc_all.at[order[i]]

    def window_of(c):
        return pl.ds(pl.multiple_of(c * rows_half, rows_half), window)

    def half_of(c):
        return pl.ds(pl.multiple_of(c * rows_half, rows_half), rows_half)

    before = pl.ds(pl.multiple_of((core * rows_half + seq - halo) % seq, halo), halo)

    def cut_one(i, part, top, picked, got, sems):
        for side in (1, 0):
            down(i, side, top)
            remote(stage.at[i, side, picked(1 - core), :], got.at[i, side], rs_send.at[sems, i, side], rs_recv.at[sems, i, side], {"tp": mate})

    def cross_one(i, picked, got, sent, there, sems):
        landed(got.at[i, 1], rs_send.at[sems, i, 1], rs_recv.at[sems, i, 1])
        sent[i] = (stage[i, 1, picked(core), :].astype(f32) + got[i, 1].astype(f32)).astype(bf16)
        remote(sent.at[i], there.at[fs_slab(i)], rs_send.at[sems, i, 2], rz_recv(sems, i), {"fs": partner})

    def fs_slab(i):
        return order[i]

    def rz_recv(sems, i):
        return rs_recv.at[sems, order[i], 2]

    def fold_one(i, picked, got, there, sent, far, sems):
        landed(got.at[i, 0], rs_send.at[sems, i, 0], rs_recv.at[sems, i, 0])
        landed(there.at[fs_slab(i)], rs_send.at[sems, i, 2], rz_recv(sems, i))
        total = stage[i, 0, picked(core), :].astype(f32) + got[i, 0].astype(f32) + there[fs_slab(i)].astype(f32)
        sent[i] = total.astype(bf16)
        remote(sent.at[i], far.at[i], rs_send.at[sems, i, 3], rs_recv.at[sems, i, 3], {"tp": across})

    def total_of(i, sent, far, sems):
        landed(far.at[i], rs_send.at[sems, i, 3], rs_recv.at[sems, i, 3])
        return 0.5 * ((sent[i].astype(f32) + far[i].astype(f32)) * scales(i)[0:1, :])

    def cut_a(i):
        cut_one(i, None, halo, window_of, rs_a, 0)

    def cross_a(i):
        cross_one(i, window_of, rs_a, s_z, rs_z, 0)

    def fold_a(i):
        fold_one(i, window_of, rs_a, rs_z, s_x, rs_x, 0)

    def gather_a(i):
        total = total_of(i, s_x, rs_x, 0)
        cols = owner_cols(i)
        r1[0:halo, cols] = total[0:halo] + jnp.where(core > 0, tok[before, cols].astype(f32), 0.0)
        r1[halo:, cols] = total[halo:] + tok[half_of(core), cols].astype(f32)

    cut_a(0)
    for u in range(PARTS[DN]):
        relay(DN, 1, u)
    cross_a(0)
    for u in range(PARTS[DN]):
        send_own(DN, 3, u, ~middle)
    for u in range(PARTS[DN]):
        relay(DN, 2, u)
    pass_mixer(1)
    rest(DN, 1)
    cut_a(1)
    cross_a(1)
    fold_a(0)
    for u in range(PARTS[DN]):
        relay(DN, 3, u)
    rest(DN, 2)
    cut_a(2)
    pass_mixer(2)
    cross_a(2)
    fold_a(1)
    rest(DN, 3)
    cut_a(3)
    pass_mixer(3)
    cross_a(3)
    gather_a(0)
    fold_a(2)
    gather_a(1)
    for k in (1, 2, 3):
        landed(ps_all.at[peers[k]], tp_send.at[2, 0, k - 1], tp_recv.at[2, 0, k - 1])
    for i in range(n):
        have_mixer(i)
    fold_a(3)
    gather_a(2)
    gather_a(3)

    second[...] = normed_rows(r1[...], gains[1:2, :])
    total = dot(second[:, owner_cols(0)], wi_all[order[0]])
    for i in range(1, n):
        total = total + dot(second[:, owner_cols(i)], wi_all[order[i]])
    values = (total * isc[...]).astype(bf16).astype(f32)
    sums = values
    position = lax.broadcasted_iota(jnp.int32, (rows_half, gc), 0) + core * rows_half
    for g in range(groups):
        span = 2 ** (g + 1)
        sums = sums + pltpu.roll(sums, span // 2, 0)
        at = slice(g * gc, (g + 1) * gc)
        counts = jnp.minimum(position + 1, span).astype(f32)
        pooled = (sums[halo:, 0:gc] / counts - values[halo:, at]).astype(bf16)
        pool[:, at] = (dot(pooled, pmap[g].astype(bf16)) * ps_all[g, 0:1, :]).astype(bf16)
        sums = sums[:, gc:]
    for i in range(n):
        cols = owner_cols(i)
        r2[:, cols] = r1[halo:, cols] + dot(pool[...], wo_all[order[i]]) * scales(i)[1:2, :]
    third[half_of(core), :] = normed_rows(r2[...], gains[2:3, :])
    wait_sent()

    def quarter(c, x):
        return pl.ds(pl.multiple_of(c * rows_half + x * share, share), share)

    def beside(c, x):
        return pl.ds(pl.multiple_of(seq + c * rows_half + x * share, share), share)

    span_cols = width // CHUNKS
    chunk = [slice(j * span_cols, (j + 1) * span_cols) for j in range(CHUNKS)]
    for j in range(CHUNKS):
        remote(third.at[quarter(core, chip), chunk[j]], third.at[beside(core, chip), chunk[j]], ag_send.at[j, 1], ag_recv.at[j, 1], {"fs": partner})
    mine = third.at[half_of(core), :]
    remote(mine, mine, ag_send.at[0, 0], ag_recv.at[0, 0], {"tp": mate})

    def hidden_rows(side):
        rows = slice(side * seq, (side + 1) * seq)

        @pl.loop(0, 2 * hu // TILE)
        def _(j):
            at = pl.ds(pl.multiple_of(j * TILE, TILE), TILE)
            acc = dot(third[rows, owner_cols(0)], held_gu(0)[:, at])
            for i in range(1, n):
                acc = acc + dot(third[rows, owner_cols(i)], held_gu(i)[:, at])
            gacc[rows, at] = acc

        activate(rows)

    def forward_third(j):
        here = third.at[beside(core, chip), chunk[j]]
        landed(here, ag_send.at[j, 1], ag_recv.at[j, 1])
        remote(here, here, ag_send.at[j, 2], ag_recv.at[j, 2], {"tp": across})
        remote(here, here, ag_send.at[j, 3], ag_recv.at[j, 3], {"tp": mate})

    def pass_third(j):
        there = third.at[beside(core, 1 - chip), chunk[j]]
        landed(there, ag_send.at[j, 2], ag_recv.at[j, 2])
        remote(there, there, ag_send.at[j, 4], ag_recv.at[j, 4], {"tp": mate})

    landed(third.at[half_of(1 - core), :], ag_send.at[0, 0], ag_recv.at[0, 0])
    hidden_rows(0)
    forward_third(0)
    for i in range(n):
        down(i, 0, 0)
        remote(stage.at[i, 0, half_of(1 - core), :], ra_2.at[i, 0], rs_send.at[1, i, 0], rs_recv.at[1, i, 0], {"tp": mate})
        if i + 1 < CHUNKS:
            forward_third(i + 1)
    for j in range(CHUNKS):
        pass_third(j)
    for j in range(CHUNKS):
        landed(third.at[beside(1 - core, chip), chunk[j]], ag_send.at[j, 3], ag_recv.at[j, 3])
        landed(third.at[beside(1 - core, 1 - chip), chunk[j]], ag_send.at[j, 4], ag_recv.at[j, 4])
    hidden_rows(1)

    def cross_b(i):
        cross_one(i, half_of, ra_2, sz_2, rz_2, 1)

    def fold_b(i):
        fold_one(i, half_of, ra_2, rz_2, sx_2, rx_2, 1)

    def final_b(i):
        total = total_of(i, sx_2, rx_2, 1)
        cols = owner_cols(i)
        out[half_of(core), cols] = (r2[:, cols] + total).astype(bf16)
        done = out.at[half_of(core), cols]
        remote(done, done, ag_send.at[i, 5], ag_recv.at[i, 5], {"tp": mate})

    for i in range(n):
        down(i, 1, 0)
        remote(stage.at[i, 1, half_of(1 - core), :], ra_2.at[i, 1], rs_send.at[1, i, 1], rs_recv.at[1, i, 1], {"tp": mate})
        if i > 0:
            cross_b(i - 1)
    cross_b(n - 1)
    for i in range(n):
        fold_b(i)
        if i > 0:
            final_b(i - 1)
    final_b(n - 1)
    for i in range(n):
        landed(out.at[half_of(1 - core), owner_cols(i)], ag_send.at[i, 5], ag_recv.at[i, 5])
    wait_sent()


def fused_layer(
    tokens, norm_gains, gate_weight, up_weight, hidden_scales, down_weight, down_scale, mix_in, in_scale,
    pool_map, pool_scale, mix_out, out_scale,
):
    n = lax.axis_size("fs")
    seq, width = tokens.shape
    slab, units = gate_weight.shape
    hu = units // 2
    groups, gc, _ = pool_map.shape
    rows_half = seq // 2
    window = rows_half + widest
    vmem = pl.BlockSpec(memory_space=pltpu.VMEM)
    dma = pltpu.SemaphoreType.DMA
    hbm = pl.BlockSpec(memory_space=pl.ANY)
    args = (
        (tokens, vmem), (norm_gains, vmem), (gate_weight, hbm), (up_weight, hbm), (hidden_scales, vmem),
        (down_weight, hbm), (mix_in, hbm), (mix_out, hbm), (in_scale[None], vmem), (pool_map, vmem),
        (pool_scale[None], vmem), (down_scale[None], vmem), (out_scale[None], vmem),
    )
    return pl.pallas_call(
        functools.partial(layer_kernel, n),
        out_shape=jax.ShapeDtypeStruct((seq, width), bf16),
        in_specs=[spec for _, spec in args],
        out_specs=vmem,
        scratch_shapes=[
            pltpu.VMEM((slab, units), f32),
            pltpu.VMEM((slab, units), f32),
            pltpu.VMEM((units, slab), f32),
            pltpu.VMEM((slab, gc), f32),
            pltpu.VMEM((gc, slab), f32),
            pltpu.VMEM((8, slab), f32),
            pltpu.VMEM((2, slab, 2 * hu), bf16),
            pltpu.VMEM((2, hu, slab), bf16),
            pltpu.VMEM((n, slab, 2 * hu), bf16),
            pltpu.VMEM((n, hu, slab), bf16),
            pltpu.VMEM((n, slab, groups * gc), bf16),
            pltpu.VMEM((n, groups * gc, slab), bf16),
            pltpu.VMEM((n, 8, slab), f32),
            pltpu.VMEM((4, 8, gc), f32),
            pltpu.VMEM((seq, width), bf16),
            pltpu.VMEM((2 * seq, width), bf16),
            pltpu.VMEM((2 * seq, 2 * hu), f32),
            pltpu.VMEM((2 * seq, hu), bf16),
            pltpu.VMEM((n, 2, seq + widest, slab), bf16),
            pltpu.VMEM((n, 2, window, slab), bf16),
            pltpu.VMEM((n, window, slab), bf16),
            pltpu.VMEM((n, window, slab), bf16),
            pltpu.VMEM((n, window, slab), bf16),
            pltpu.VMEM((n, window, slab), bf16),
            pltpu.VMEM((window, width), f32),
            pltpu.VMEM((window, width), bf16),
            pltpu.VMEM((rows_half, groups * gc), bf16),
            pltpu.VMEM((rows_half, width), f32),
            pltpu.VMEM((2 * seq, width), bf16),
            pltpu.VMEM((n, 2, rows_half, slab), bf16),
            pltpu.VMEM((n, rows_half, slab), bf16),
            pltpu.VMEM((n, rows_half, slab), bf16),
            pltpu.VMEM((n, rows_half, slab), bf16),
            pltpu.VMEM((n, rows_half, slab), bf16),
            dma((n - 1, FIRST_PART[-1])), dma((2, n, FIRST_PART[-1])), dma((n, 2 * FIRST_PART[-1])),
            dma((n - 1,)), dma((n,)),
            dma((3, n, 3)), dma((3, n, 3)),
            dma((4,)), dma((4,)),
            dma((2, n, 4)), dma((2, n, 4)),
            dma((n, 6)), dma((n, 6)),
            dma((7,)),
        ],
        compiler_params=pltpu.CompilerParams(
            collective_id=0, has_side_effects=True, vmem_limit_bytes=60 * 1024 * 1024
        ),
    )(*[value for value, _ in args])


def solution(mesh):
    body = fused_layer if fits_kernel(mesh) else per_device
    return jax.shard_map(
        body,
        mesh=mesh,
        in_specs=(
            P(("rep", "fs"), None),
            P(),
            P("fs", "tp"),
            P("fs", "tp"),
            P(None, "tp"),
            P("tp", "fs"),
            P("fs"),
            P("fs", None),
            P(),
            P(),
            P("tp"),
            P("tp", "fs"),
            P("fs"),
        ),
        out_specs=P(("rep", "fs"), None),
        check_vma=False,
    )
```

```python
import functools

import jax
import jax.numpy as jnp
from jax import lax
from jax.experimental import pallas as pl
from jax.experimental.pallas import tpu as pltpu
from jax.sharding import PartitionSpec as P

eps = 1e-06
widest = 16


def normed(values, gain):
    mean_sq = jnp.mean(values * values, axis=-1, keepdims=True)
    return (values * lax.rsqrt(mean_sq + eps) * gain).astype(jnp.bfloat16)


def scatter_rows(term_fn, share):
    return lax.psum_scatter(
        term_fn(jnp.int32(0), lax.axis_size("tp") * share).astype(jnp.bfloat16),
        "tp",
        scatter_dimension=0,
        tiled=True,
    ).astype(jnp.float32)


def whole_rows(values):
    return lax.all_gather(values, "tp", axis=0, tiled=True)


def fetch_mixer(in_cols, mix_out):
    return (
        lax.all_gather(in_cols.astype(jnp.bfloat16), "fs", axis=0, tiled=True),
        lax.all_gather(mix_out.astype(jnp.bfloat16), "fs", axis=1, tiled=True),
    )


def hidden_units(rows_in, gate_full, up_full, hidden_scales):
    gate = jnp.dot(rows_in, gate_full, preferred_element_type=jnp.float32) * hidden_scales[0]
    upper = jnp.dot(rows_in, up_full, preferred_element_type=jnp.float32) * hidden_scales[1]
    return (jax.nn.silu(gate) * upper).astype(jnp.bfloat16)


def ffn_partial(normed_rows, gate_full, up_full, down_full, hidden_scales, share):

    def term_rows(row_start, row_count):
        hidden = hidden_units(normed_rows, gate_full, up_full, hidden_scales)
        return jnp.dot(hidden, down_full, preferred_element_type=jnp.float32)

    return scatter_rows(term_rows, share)


def per_device(
    tokens,
    norm_gains,
    gate_weight,
    up_weight,
    hidden_scales,
    down_weight,
    down_scale,
    mix_in,
    in_scale,
    pool_map,
    pool_scale,
    mix_out,
    out_scale,
):
    tp_width = lax.axis_size("tp")
    tp_rank = lax.axis_index("tp")
    seq_rows = tokens.shape[0]
    share = seq_rows // tp_width
    local_channels = mix_out.shape[0]
    group_width = pool_map.shape[1]
    needed = max(group_width, local_channels)
    first_channel = tp_rank * local_channels
    in_start = first_channel // group_width * group_width
    in_cols = lax.dynamic_slice_in_dim(mix_in, in_start, needed, 1)
    scale_cols = lax.dynamic_slice_in_dim(in_scale, in_start, needed, 0)
    down_cols, out_cols = (
        lax.all_gather(down_scale, "fs", axis=0, tiled=True),
        lax.all_gather(out_scale, "fs", axis=0, tiled=True),
    )
    gate_bf = gate_weight.astype(jnp.bfloat16)
    up_bf = up_weight.astype(jnp.bfloat16)
    down_bf = down_weight.astype(jnp.bfloat16)
    resid_all = tokens.astype(jnp.float32)
    first = normed(resid_all, norm_gains[0])
    gate_full, up_full, down_full = (
        lax.all_gather(gate_bf, "fs", axis=0, tiled=True),
        lax.all_gather(up_bf, "fs", axis=0, tiled=True),
        lax.all_gather(down_bf, "fs", axis=1, tiled=True),
    )
    ffn_one = ffn_partial(first, gate_full, up_full, down_full, hidden_scales, share)
    own_rows = lax.dynamic_slice_in_dim(resid_all, tp_rank * share, share, 0)
    resid_one = own_rows + 0.5 * (ffn_one * down_cols)
    second = whole_rows(normed(resid_one, norm_gains[1]))
    in_full, out_full = fetch_mixer(in_cols, mix_out)
    pool_in = (jnp.dot(second, in_full, preferred_element_type=jnp.float32) * scale_cols).astype(
        jnp.bfloat16
    )
    channel = in_start + jnp.arange(needed, dtype=jnp.int32)
    window = jnp.left_shift(jnp.int32(2), channel // group_width)
    position = jnp.arange(seq_rows, dtype=jnp.int32)[:, None]
    values = pool_in.astype(jnp.float32)
    summed = jnp.zeros_like(values)
    for offset in range(widest):
        shifted = jnp.pad(values, ((offset, 0), (0, 0)))[:seq_rows]
        summed = summed + jnp.where(offset < window, shifted, 0.0)
    counts = jnp.minimum(position + 1, window).astype(jnp.float32)
    pooled = (summed / counts - values).astype(jnp.bfloat16)
    map_bf = pool_map.astype(jnp.bfloat16)
    if local_channels < group_width:
        group_index = first_channel // group_width
        column_start = first_channel % group_width
        map_cols = lax.dynamic_slice(
            map_bf, (group_index, jnp.int32(0), column_start), (1, group_width, local_channels)
        )[0]
        grouped = jnp.dot(pooled, map_cols, preferred_element_type=jnp.float32)
    else:
        held_groups = local_channels // group_width
        maps_held = lax.dynamic_slice_in_dim(map_bf, first_channel // group_width, held_groups, 0)
        grouped = jnp.einsum(
            "tgc,gcd->tgd",
            pooled.reshape(seq_rows, held_groups, group_width),
            maps_held,
            preferred_element_type=jnp.float32,
        ).reshape(seq_rows, local_channels)
    pool_out = (grouped * pool_scale).astype(jnp.bfloat16)

    def mixer_rows(row_start, row_count):
        return jnp.dot(pool_out, out_full, preferred_element_type=jnp.float32)

    mixed = scatter_rows(mixer_rows, share)
    resid_two = resid_one + mixed * out_cols
    third = whole_rows(normed(resid_two, norm_gains[2]))
    ffn_two = ffn_partial(third, gate_full, up_full, down_full, hidden_scales, share)
    final_rows = (resid_two + 0.5 * (ffn_two * down_cols)).astype(jnp.bfloat16)
    return whole_rows(final_rows)


MESH = pl.DeviceIdType.MESH
PARTS = (1, 1, 4, 4)
FIRST_PART = (0, 1, 2, 6, 10)
TILE = 256
BATCHES = 2
MIXER_AFTER = 1
bf16 = jnp.bfloat16
f32 = jnp.float32


def fits_kernel(mesh):
    return mesh.shape["rep"] == 2 and mesh.shape["fs"] == 4 and mesh.shape["tp"] == 4


def layer_kernel(
    n, tok, gains, gate_hbm, up_hbm, hs, down_hbm, mix_in_hbm, mix_out_hbm, isc, pmap, pool_scale, down_scale, out_scale,
    out, wide_gate, wide_up, wide_down, wide_in, wide_out, sc_in, gu_own, dn_own, gu_buf, dn_buf, wi_all, wo_all, sc_all, ps_all,
    ptok, first, gacc, hidden, stage, rs_a, s_z, rs_z, s_x, rs_x, r1, second, pool, r2, third, stage_2, ra_2, sz_2, rz_2, sx_2, rx_2,
    z_send, y_send, w_recv, sc_send, sc_recv, tp_send, tp_recv, tk_send, tk_recv, rs_send, rs_recv, rt_send, rt_recv, ag_send, ag_recv, loc,
):
    rep, fs, me = lax.axis_index("rep"), lax.axis_index("fs"), lax.axis_index("tp")
    seq, width = tok.shape
    slab = width // n
    share = seq // 4
    rows_half = seq // 2
    halo = widest
    window = rows_half + halo
    units = hs.shape[1]
    hu = units // 2
    groups, gc = pmap.shape[0], pmap.shape[1]
    core, chip = me % 2, me // 2
    mate = me + 1 - 2 * core
    across = (me + 2) % 4
    diag = (mate + 2) % 4
    peers = {1: mate, 2: across, 3: diag}
    partner = fs + 1 - 2 * (fs % 2)
    far_mid = jnp.where(fs < 2, 2, 1)
    far_end = jnp.where(fs < 2, 3, 0)
    order = (fs, partner, far_mid, far_end)
    middle = (fs == 1) | (fs == 2)
    kind = jnp.where(middle, 1, 0)
    kind_of = (kind, 1 - kind, 1, 0)

    def owner_cols(i):
        return pl.ds(pl.multiple_of(order[i] * slab, slab), slab)

    def cols_of(rank):
        return pl.ds(pl.multiple_of(rank * gc, gc), gc)

    half = slab // 2
    mine_half = pl.ds(pl.multiple_of(rep * half, half), half)
    other_half = pl.ds(pl.multiple_of((1 - rep) * half, half), half)
    loads = [
        pltpu.make_async_copy(mix_in_hbm.at[:, cols_of(me)], wide_in, loc.at[0]),
        pltpu.make_async_copy(mix_out_hbm, wide_out, loc.at[1]),
        pltpu.make_async_copy(gate_hbm.at[mine_half, :], wide_gate.at[mine_half, :], loc.at[2]),
        pltpu.make_async_copy(up_hbm.at[mine_half, :], wide_up.at[mine_half, :], loc.at[3]),
        pltpu.make_async_copy(gate_hbm.at[other_half, :], wide_gate.at[other_half, :], loc.at[4]),
        pltpu.make_async_copy(up_hbm.at[other_half, :], wide_up.at[other_half, :], loc.at[5]),
        pltpu.make_async_copy(down_hbm, wide_down, loc.at[6]),
    ]
    for load in loads:
        load.start()
    barrier = pltpu.get_barrier_semaphore()
    for i in (1, 2, 3):
        pl.semaphore_signal(barrier, inc=1, device_id={"fs": order[i]}, device_id_type=MESH)
    for k in (1, 2, 3):
        pl.semaphore_signal(barrier, inc=1, device_id={"tp": peers[k]}, device_id_type=MESH)
    pl.semaphore_signal(barrier, inc=1, device_id={"rep": 1 - rep}, device_id_type=MESH)

    sc_in[...] = jnp.zeros_like(sc_in)
    sc_in[0:1, :] = down_scale[...]
    sc_in[1:2, :] = out_scale[...]
    ps_all[me] = jnp.broadcast_to(pool_scale[...], ps_all.shape[1:])

    WI, WO, GU, DN = range(4)

    def piece(t, i, at, own_kind=None):
        shard = order[i]
        if t == WI:
            return wi_all.at[shard, pl.ds(pl.multiple_of(at * half, half), half), cols_of(me)]
        if t == WO:
            rows = gc // 2
            return wo_all.at[shard, pl.ds(pl.multiple_of(me * gc + at * rows, rows), rows), :]
        ref = (gu_own if t == GU else dn_own).at[own_kind] if own_kind is not None else (gu_buf if t == GU else dn_buf).at[shard]
        rows = ref.shape[0] // (2 * PARTS[t])
        return ref.at[pl.ds(pl.multiple_of(at * rows, rows), rows), :]

    started = []

    def start_if(cond, copy):
        if cond is None:
            copy.start()
        else:
            @pl.when(cond)
            def _():
                copy.start()
        started.append((cond, copy))

    def wait_sent():
        for cond, copy in started:
            if cond is None:
                copy.wait_send()
            else:
                @pl.when(cond)
                def _():
                    copy.wait_send()
        started.clear()

    def remote(src, dst, s_sem, r_sem, dev, cond=None):
        start_if(cond, pltpu.make_async_remote_copy(
            src_ref=src, dst_ref=dst, send_sem=s_sem, recv_sem=r_sem, device_id=dev, device_id_type=MESH
        ))

    def landed(dst, s_sem, r_sem):
        pltpu.make_async_remote_copy(
            src_ref=dst, dst_ref=dst, send_sem=s_sem, recv_sem=r_sem, device_id={"tp": mate}, device_id_type=MESH
        ).wait_recv()

    def send_own(t, i, u, cond=None):
        at = rep * PARTS[t] + u
        remote(
            piece(t, 0, at, kind_of[i] if t >= GU else None), piece(t, 0, at),
            z_send.at[i - 1, FIRST_PART[t] + u], w_recv.at[fs, 2 * FIRST_PART[t] + at], {"fs": order[i]}, cond,
        )

    def arrived(t, i, at):
        landed(piece(t, i, at), z_send.at[0, 0], w_recv.at[order[i], 2 * FIRST_PART[t] + at])

    def relay(t, i, u):
        at = rep * PARTS[t] + u
        arrived(t, i, at)
        here = piece(t, i, at)
        sem = w_recv.at[order[i], 2 * FIRST_PART[t] + at]
        if t < GU and i > 1:
            remote(here, here, y_send.at[0, i, FIRST_PART[t] + u], sem, {"fs": partner}, middle)
        remote(here, here, y_send.at[1, i, FIRST_PART[t] + u], sem, {"rep": 1 - rep})

    def rest(t, i):
        for u in range(PARTS[t]):
            arrived(t, i, (1 - rep) * PARTS[t] + u)

    loads[0].wait()
    loads[1].wait()
    wi_all[fs, :, cols_of(me)] = wide_in[...].astype(bf16)
    wo_all[fs, pl.ds(pl.multiple_of(me * gc, gc), gc), :] = wide_out[...].astype(bf16)

    def cast_gate_up(start, count, kinds):
        @pl.loop(0, count // 32)
        def _(j):
            rows = pl.ds(pl.multiple_of(start + j * 32, 32), 32)
            for h in kinds:
                cols = pl.ds(h * hu if isinstance(h, int) else pl.multiple_of(h * hu, 128), hu)
                gu_own[h, rows, 0:hu] = wide_gate[rows, cols].astype(bf16)
                gu_own[h, rows, hu:] = wide_up[rows, cols].astype(bf16)

    def my_rows(rank):
        return pl.ds(pl.multiple_of(rank * share, share), share)

    pl.semaphore_wait(barrier, n - 1 + 4)
    remote(tok.at[my_rows(me), :], ptok.at[my_rows(me), :], tk_send.at[0], tk_recv.at[0], {"fs": partner})
    loads[2].wait()
    loads[3].wait()
    for u in range(PARTS[GU]):
        cast_gate_up(rep * half + u * (half // PARTS[GU]), half // PARTS[GU], (0, 1))
        for i in (3, 2, 1):
            send_own(GU, i, u)
        if u == MIXER_AFTER:
            for t in (WI, WO):
                for i in (2, 1):
                    send_own(t, i, 0)

    def spread(t, i, rank):
        return wi_all.at[order[i], :, cols_of(rank)] if t == WI else wo_all.at[order[i], pl.ds(pl.multiple_of(rank * gc, gc), gc), :]

    def share_mixer(i):
        for t in (WI, WO):
            mine = spread(t, i, me)
            remote(mine, mine, tp_send.at[t, i, 1], tp_recv.at[t, i, 1], {"tp": across})
            remote(mine, mine, tp_send.at[t, i, 0], tp_recv.at[t, i, 0], {"tp": mate})

    def pass_mixer(i):
        for t in (WI, WO):
            theirs = spread(t, i, across)
            landed(theirs, tp_send.at[t, i, 1], tp_recv.at[t, i, 1])
            remote(theirs, theirs, tp_send.at[t, i, 2], tp_recv.at[t, i, 2], {"tp": mate})

    def have_mixer(i):
        for t in (WI, WO):
            landed(spread(t, i, mate), tp_send.at[t, i, 0], tp_recv.at[t, i, 0])
            landed(spread(t, i, diag), tp_send.at[t, i, 2], tp_recv.at[t, i, 2])

    share_mixer(0)
    loads[4].wait()
    loads[5].wait()
    cast_gate_up((1 - rep) * half, half, (kind,))
    loads[6].wait()

    @pl.loop(0, hu // 32)
    def _(j):
        rows = pl.ds(pl.multiple_of(j * 32, 32), 32)
        for h in (0, 1):
            dn_own[h, rows, :] = wide_down[pl.ds(pl.multiple_of(h * hu + j * 32, 32), 32), :].astype(bf16)

    for i in (1, 2, 3):
        remote(sc_in, sc_all.at[fs], sc_send.at[i - 1], sc_recv.at[fs], {"fs": order[i]})
    for k in (1, 2, 3):
        remote(ps_all.at[me], ps_all.at[me], tp_send.at[2, 0, k - 1], tp_recv.at[2, 0, k - 1], {"tp": peers[k]})

    def normed_rows(values, gain):
        mean_sq = jnp.mean(values * values, axis=-1, keepdims=True)
        return (values * lax.rsqrt(mean_sq + eps) * gain).astype(bf16)

    stage[:, :, 0:halo, :] = jnp.zeros((n, 2, halo, slab), bf16)

    def norm_first(source, top):
        @pl.loop(0, seq // 32)
        def _(j):
            rows = pl.ds(pl.multiple_of(j * 32, 32), 32)
            first[pl.ds(pl.multiple_of(top + j * 32, 32), 32), :] = normed_rows(source[rows, :].astype(f32), gains[0:1, :])

    def dot(a, b):
        return jnp.dot(a, b, preferred_element_type=f32)

    def held_gu(i):
        return gu_own.at[kind] if i == 0 else gu_buf.at[order[i]]

    def held_dn(i):
        return dn_own.at[kind] if i == 0 else dn_buf.at[order[i]]

    def gate_up(i, fresh):
        weights = held_gu(i)
        cols = owner_cols(i)

        @pl.loop(0, 2 * hu // TILE)
        def _(j):
            at = pl.ds(pl.multiple_of(j * TILE, TILE), TILE)
            term = dot(first[:, cols], weights[:, at])
            if fresh:
                gacc[:, at] = term
            else:
                gacc[:, at] += term

    def activate(rows):
        @pl.loop(0, hu // 128)
        def _(j):
            at = pl.ds(pl.multiple_of(j * 128, 128), 128)
            up_at = pl.ds(pl.multiple_of(hu + j * 128, 128), 128)
            sc_at = pl.ds(pl.multiple_of(kind * hu + j * 128, 128), 128)
            gate = gacc[rows, at] * hs[0:1, sc_at]
            upper = gacc[rows, up_at] * hs[1:2, sc_at]
            hidden[rows, at] = (gate / (1.0 + jnp.exp(-gate)) * upper).astype(bf16)

    def down(i, side):
        weights = held_dn(i)

        @pl.loop(0, slab // TILE)
        def _(j):
            at = pl.ds(pl.multiple_of(j * TILE, TILE), TILE)
            stage[i, side, halo:, at] = dot(hidden[side * seq:(side + 1) * seq, :], weights[:, at]).astype(bf16)

    norm_first(tok, 0)
    own_rows = my_rows(me)
    landed(ptok.at[own_rows, :], tk_send.at[0], tk_recv.at[0])
    for k in (2, 3, 1):
        remote(ptok.at[own_rows, :], ptok.at[own_rows, :], tk_send.at[k], tk_recv.at[k], {"tp": peers[k]})
    def relay_mixer(i):
        for t in (WI, WO):
            relay(t, i, 0)

    def rest_mixer(i):
        rest(WI, i)
        rest(WO, i)
        share_mixer(i)

    for u in range(PARTS[GU]):
        for i in (1, 2, 3):
            relay(GU, i, u)
        if u == 1:
            for k in (1, 2, 3):
                landed(ptok.at[my_rows(peers[k]), :], tk_send.at[k], tk_recv.at[k])
            norm_first(ptok, seq)
        if u == 2:
            relay_mixer(1)
            for i in (1, 2, 3):
                for v in range(PARTS[DN]):
                    send_own(DN, i, v, middle if i == 3 else None)
            gate_up(0, True)
    relay_mixer(2)
    relay_mixer(3)
    rest_mixer(1)
    rest(GU, 1)
    gate_up(1, False)
    pass_mixer(0)
    rest(GU, 2)
    gate_up(2, False)
    rest_mixer(2)
    rest_mixer(3)
    rest(GU, 3)
    gate_up(3, False)
    activate(slice(None))

    for i in (1, 2, 3):
        landed(sc_all.at[order[i]], sc_send.at[0], sc_recv.at[order[i]])

    def scales(i):
        return sc_in if i == 0 else sc_all.at[order[i]]

    def half_of(c):
        return pl.ds(pl.multiple_of(c * rows_half, rows_half), rows_half)

    before = pl.ds(pl.multiple_of((core * rows_half + seq - halo) % seq, halo), halo)
    batch = rows_half // BATCHES
    whole = ((0, window),)
    split = tuple((b * batch + (halo if b else 0), batch + (0 if b else halo)) for b in range(BATCHES))

    def parts(i):
        return split if i == n - 1 else whole

    def window_of(c, part):
        return pl.ds(pl.multiple_of(c * rows_half + part[0], halo), part[1])

    def cut_a(i):
        for side in (1, 0):
            down(i, side)
            for p, part in enumerate(parts(i)):
                remote(
                    stage.at[i, side, window_of(1 - core, part), :], rs_a.at[i, side, pl.ds(*part), :],
                    rs_send.at[p, i, side], rs_recv.at[p, i, side], {"tp": mate},
                )

    def cross_a(i):
        for p, part in enumerate(parts(i)):
            rows = pl.ds(*part)
            landed(rs_a.at[i, 1, rows, :], rs_send.at[p, i, 1], rs_recv.at[p, i, 1])
            s_z[i, rows, :] = (stage[i, 1, window_of(core, part), :].astype(f32) + rs_a[i, 1, rows, :].astype(f32)).astype(bf16)
            remote(
                s_z.at[i, rows, :], rs_z.at[order[i], rows, :], rs_send.at[p, i, 2], rs_recv.at[p, order[i], 2], {"fs": partner}
            )

    def fold_a(i, p=0):
        part = parts(i)[p]
        rows = pl.ds(*part)
        landed(rs_a.at[i, 0, rows, :], rs_send.at[p, i, 0], rs_recv.at[p, i, 0])
        landed(rs_z.at[order[i], rows, :], rs_send.at[p, i, 2], rs_recv.at[p, order[i], 2])
        total = stage[i, 0, window_of(core, part), :].astype(f32) + rs_a[i, 0, rows, :].astype(f32)
        s_x[i, rows, :] = (total + rs_z[order[i], rows, :].astype(f32)).astype(bf16)
        remote(s_x.at[i, rows, :], rs_x.at[i, rows, :], rs_send.at[p, i, 3], rs_recv.at[p, i, 3], {"tp": across})

    def gather_a(i, p=0):
        part = parts(i)[p]
        top, count = part
        rows = pl.ds(*part)
        landed(rs_x.at[i, rows, :], rs_send.at[p, i, 3], rs_recv.at[p, i, 3])
        total = 0.5 * ((s_x[i, rows, :].astype(f32) + rs_x[i, rows, :].astype(f32)) * scales(i)[0:1, :])
        cols = owner_cols(i)
        if top == 0:
            r1[0:halo, cols] = total[0:halo] + jnp.where(core > 0, tok[before, cols].astype(f32), 0.0)
            total, top, count = total[halo:], halo, count - halo
        held = pl.ds(pl.multiple_of(core * rows_half + top - halo, halo), count)
        r1[top:top + count, cols] = total + tok[held, cols].astype(f32)

    cut_a(0)
    for u in range(PARTS[DN]):
        relay(DN, 1, u)
    cross_a(0)
    for u in range(PARTS[DN]):
        send_own(DN, 3, u, ~middle)
    for u in range(PARTS[DN]):
        relay(DN, 2, u)
    pass_mixer(1)
    rest(DN, 1)
    cut_a(1)
    cross_a(1)
    fold_a(0)
    for u in range(PARTS[DN]):
        relay(DN, 3, u)
    rest(DN, 2)
    cut_a(2)
    pass_mixer(2)
    cross_a(2)
    fold_a(1)
    rest(DN, 3)
    cut_a(3)
    pass_mixer(3)
    cross_a(3)
    gather_a(0)
    fold_a(2)
    gather_a(1)
    for k in (1, 2, 3):
        landed(ps_all.at[peers[k]], tp_send.at[2, 0, k - 1], tp_recv.at[2, 0, k - 1])
    for i in range(n):
        have_mixer(i)
    gather_a(2)

    def mixer(b):
        low = b * batch
        taken = slice(low, low + batch + halo)
        second[...] = normed_rows(r1[taken, :], gains[1:2, :])
        total = dot(second[:, owner_cols(0)], wi_all[order[0]])
        for i in range(1, n):
            total = total + dot(second[:, owner_cols(i)], wi_all[order[i]])
        values = (total * isc[...]).astype(bf16).astype(f32)
        sums = values
        position = lax.broadcasted_iota(jnp.int32, (batch, gc), 0) + (core * rows_half + low)
        for g in range(groups):
            span = 2 ** (g + 1)
            sums = sums + pltpu.roll(sums, span // 2, 0)
            at = slice(g * gc, (g + 1) * gc)
            counts = jnp.minimum(position + 1, span).astype(f32)
            pooled = (sums[halo:, 0:gc] / counts - values[halo:, at]).astype(bf16)
            pool[:, at] = (dot(pooled, pmap[g].astype(bf16)) * ps_all[g, 0:1, :]).astype(bf16)
            sums = sums[:, gc:]
        rows = slice(low, low + batch)
        for i in range(n):
            cols = owner_cols(i)
            r2[rows, cols] = r1[low + halo:low + halo + batch, cols] + dot(pool[...], wo_all[order[i]]) * scales(i)[1:2, :]
        third[lot(b, 0, core), :] = normed_rows(r2[rows, :], gains[2:3, :])

    def lot(b, side, c):
        return pl.ds(pl.multiple_of(((b * 2 + side) * 2 + c) * batch, batch), batch)

    def piece_of(b, side, c, x):
        return pl.ds(pl.multiple_of(((b * 2 + side) * 2 + c) * batch + x * (batch // 2), batch // 2), batch // 2)

    def both(b, side):
        return slice((b * 2 + side) * 2 * batch, (b * 2 + side + 1) * 2 * batch)

    def send_third(b):
        remote(third.at[piece_of(b, 0, core, chip), :], third.at[piece_of(b, 1, core, chip), :], ag_send.at[b, 1], ag_recv.at[b, 1], {"fs": partner})
        mine = third.at[lot(b, 0, core), :]
        remote(mine, mine, ag_send.at[b, 0], ag_recv.at[b, 0], {"tp": mate})

    def have_own(b):
        landed(third.at[lot(b, 0, 1 - core), :], ag_send.at[b, 0], ag_recv.at[b, 0])

    def forward_third(b):
        here = third.at[piece_of(b, 1, core, chip), :]
        landed(here, ag_send.at[b, 1], ag_recv.at[b, 1])
        remote(here, here, ag_send.at[b, 2], ag_recv.at[b, 2], {"tp": across})
        remote(here, here, ag_send.at[b, 3], ag_recv.at[b, 3], {"tp": mate})

    def pass_third(b):
        there = third.at[piece_of(b, 1, core, 1 - chip), :]
        landed(there, ag_send.at[b, 2], ag_recv.at[b, 2])
        remote(there, there, ag_send.at[b, 4], ag_recv.at[b, 4], {"tp": mate})

    def have_partner(b):
        landed(third.at[piece_of(b, 1, 1 - core, chip), :], ag_send.at[b, 3], ag_recv.at[b, 3])
        landed(third.at[piece_of(b, 1, 1 - core, 1 - chip), :], ag_send.at[b, 4], ag_recv.at[b, 4])

    def hidden_rows(b, side):
        rows = both(b, side)

        @pl.loop(0, 2 * hu // TILE)
        def _(j):
            at = pl.ds(pl.multiple_of(j * TILE, TILE), TILE)
            acc = dot(third[rows, owner_cols(0)], held_gu(0)[:, at])
            for i in range(1, n):
                acc = acc + dot(third[rows, owner_cols(i)], held_gu(i)[:, at])
            gacc[rows, at] = acc

        activate(rows)

    def down_send(i, b, side):
        rows = both(b, side)
        stage_2[i, rows, :] = dot(hidden[rows, :], held_dn(i)[...]).astype(bf16)
        remote(stage_2.at[i, lot(b, side, 1 - core), :], ra_2.at[i, b, side], rt_send.at[i, b, side], rt_recv.at[i, b, side], {"tp": mate})

    def cross_b(i, b):
        landed(ra_2.at[i, b, 1], rt_send.at[i, b, 1], rt_recv.at[i, b, 1])
        sz_2[i, b] = (stage_2[i, lot(b, 1, core), :].astype(f32) + ra_2[i, b, 1].astype(f32)).astype(bf16)
        remote(sz_2.at[i, b], rz_2.at[order[i], b], rt_send.at[i, b, 2], rt_recv.at[order[i], b, 2], {"fs": partner})

    def fold_b(i, b):
        landed(ra_2.at[i, b, 0], rt_send.at[i, b, 0], rt_recv.at[i, b, 0])
        landed(rz_2.at[order[i], b], rt_send.at[i, b, 2], rt_recv.at[order[i], b, 2])
        total = stage_2[i, lot(b, 0, core), :].astype(f32) + ra_2[i, b, 0].astype(f32) + rz_2[order[i], b].astype(f32)
        sx_2[i, b] = total.astype(bf16)
        remote(sx_2.at[i, b], rx_2.at[i, b], rt_send.at[i, b, 3], rt_recv.at[i, b, 3], {"tp": across})

    def out_rows(b, c):
        return pl.ds(pl.multiple_of(c * rows_half + b * batch, batch), batch)

    def final_b(i, b):
        landed(rx_2.at[i, b], rt_send.at[i, b, 3], rt_recv.at[i, b, 3])
        total = 0.5 * ((sx_2[i, b].astype(f32) + rx_2[i, b].astype(f32)) * scales(i)[0:1, :])
        cols = owner_cols(i)
        out[out_rows(b, core), cols] = (r2[b * batch:(b + 1) * batch, cols] + total).astype(bf16)
        done = out.at[out_rows(b, core), cols]
        remote(done, done, rt_send.at[i, b, 4], rt_recv.at[i, b, 4], {"tp": mate})

    for b in range(BATCHES):
        if b == 0:
            for q in range(BATCHES):
                fold_a(n - 1, q)
        gather_a(n - 1, b)
        mixer(b)
        send_third(b)
    have_own(0)
    hidden_rows(0, 0)
    forward_third(0)
    have_own(1)
    hidden_rows(1, 0)
    forward_third(1)
    pass_third(0)
    for i in range(n):
        down_send(i, 0, 0)
    have_partner(0)
    hidden_rows(0, 1)
    for i in range(n):
        down_send(i, 0, 1)
    pass_third(1)
    for i in range(n):
        cross_b(i, 0)
    for i in range(n):
        down_send(i, 1, 0)
    have_partner(1)
    hidden_rows(1, 1)
    for i in range(n):
        down_send(i, 1, 1)
    fold_b(0, 0)
    for i in range(n):
        cross_b(i, 1)
        if i + 1 < n:
            fold_b(i + 1, 0)
            final_b(i, 0)
    fold_b(0, 1)
    final_b(n - 1, 0)
    for i in range(n):
        if i + 1 < n:
            fold_b(i + 1, 1)
        final_b(i, 1)
    for b in range(BATCHES):
        for i in range(n):
            landed(out.at[out_rows(b, 1 - core), owner_cols(i)], rt_send.at[i, b, 4], rt_recv.at[i, b, 4])
    wait_sent()


def fused_layer(
    tokens, norm_gains, gate_weight, up_weight, hidden_scales, down_weight, down_scale, mix_in, in_scale,
    pool_map, pool_scale, mix_out, out_scale,
):
    n = lax.axis_size("fs")
    seq, width = tokens.shape
    slab, units = gate_weight.shape
    hu = units // 2
    groups, gc, _ = pool_map.shape
    rows_half = seq // 2
    window = rows_half + widest
    batch = rows_half // BATCHES
    vmem = pl.BlockSpec(memory_space=pltpu.VMEM)
    dma = pltpu.SemaphoreType.DMA
    hbm = pl.BlockSpec(memory_space=pl.ANY)
    args = (
        (tokens, vmem), (norm_gains, vmem), (gate_weight, hbm), (up_weight, hbm), (hidden_scales, vmem),
        (down_weight, hbm), (mix_in, hbm), (mix_out, hbm), (in_scale[None], vmem), (pool_map, vmem),
        (pool_scale[None], vmem), (down_scale[None], vmem), (out_scale[None], vmem),
    )
    return pl.pallas_call(
        functools.partial(layer_kernel, n),
        out_shape=pltpu.VMEM((seq, width), bf16),
        in_specs=[spec for _, spec in args],
        out_specs=vmem,
        scratch_shapes=[
            pltpu.VMEM((slab, units), f32),
            pltpu.VMEM((slab, units), f32),
            pltpu.VMEM((units, slab), f32),
            pltpu.VMEM((slab, gc), f32),
            pltpu.VMEM((gc, slab), f32),
            pltpu.VMEM((8, slab), f32),
            pltpu.VMEM((2, slab, 2 * hu), bf16),
            pltpu.VMEM((2, hu, slab), bf16),
            pltpu.VMEM((n, slab, 2 * hu), bf16),
            pltpu.VMEM((n, hu, slab), bf16),
            pltpu.VMEM((n, slab, groups * gc), bf16),
            pltpu.VMEM((n, groups * gc, slab), bf16),
            pltpu.VMEM((n, 8, slab), f32),
            pltpu.VMEM((4, 8, gc), f32),
            pltpu.VMEM((seq, width), bf16),
            pltpu.VMEM((2 * seq, width), bf16),
            pltpu.VMEM((2 * seq, 2 * hu), f32),
            pltpu.VMEM((2 * seq, hu), bf16),
            pltpu.VMEM((n, 2, seq + widest, slab), bf16),
            pltpu.VMEM((n, 2, window, slab), bf16),
            pltpu.VMEM((n, window, slab), bf16),
            pltpu.VMEM((n, window, slab), bf16),
            pltpu.VMEM((n, window, slab), bf16),
            pltpu.VMEM((n, window, slab), bf16),
            pltpu.VMEM((window, width), f32),
            pltpu.VMEM((batch + widest, width), bf16),
            pltpu.VMEM((batch, groups * gc), bf16),
            pltpu.VMEM((rows_half, width), f32),
            pltpu.VMEM((2 * seq, width), bf16),
            pltpu.VMEM((n, 2 * seq, slab), bf16),
            pltpu.VMEM((n, BATCHES, 2, batch, slab), bf16),
            pltpu.VMEM((n, BATCHES, batch, slab), bf16),
            pltpu.VMEM((n, BATCHES, batch, slab), bf16),
            pltpu.VMEM((n, BATCHES, batch, slab), bf16),
            pltpu.VMEM((n, BATCHES, batch, slab), bf16),
            dma((n - 1, FIRST_PART[-1])), dma((2, n, FIRST_PART[-1])), dma((n, 2 * FIRST_PART[-1])),
            dma((n - 1,)), dma((n,)),
            dma((3, n, 3)), dma((3, n, 3)),
            dma((4,)), dma((4,)),
            dma((BATCHES, n, 4)), dma((BATCHES, n, 4)),
            dma((n, BATCHES, 5)), dma((n, BATCHES, 5)),
            dma((BATCHES, 5)), dma((BATCHES, 5)),
            dma((7,)),
        ],
        compiler_params=pltpu.CompilerParams(
            collective_id=0, has_side_effects=True, vmem_limit_bytes=62 * 1024 * 1024
        ),
    )(*[value for value, _ in args])


def solution(mesh):
    body = fused_layer if fits_kernel(mesh) else per_device
    return jax.shard_map(
        body,
        mesh=mesh,
        in_specs=(
            P(("rep", "fs"), None),
            P(),
            P("fs", "tp"),
            P("fs", "tp"),
            P(None, "tp"),
            P("tp", "fs"),
            P("fs"),
            P("fs", None),
            P(),
            P(),
            P("tp"),
            P("tp", "fs"),
            P("fs"),
        ),
        out_specs=P(("rep", "fs"), None),
        check_vma=False,
    )
```

```python
import functools

import jax
import jax.numpy as jnp
from jax import lax
from jax.experimental import pallas as pl
from jax.experimental.pallas import tpu as pltpu
from jax.sharding import PartitionSpec as P

eps = 1e-06
widest = 16


def normed(values, gain):
    mean_sq = jnp.mean(values * values, axis=-1, keepdims=True)
    return (values * lax.rsqrt(mean_sq + eps) * gain).astype(jnp.bfloat16)


def scatter_rows(term_fn, share):
    return lax.psum_scatter(
        term_fn(jnp.int32(0), lax.axis_size("tp") * share).astype(jnp.bfloat16),
        "tp",
        scatter_dimension=0,
        tiled=True,
    ).astype(jnp.float32)


def whole_rows(values):
    return lax.all_gather(values, "tp", axis=0, tiled=True)


def fetch_mixer(in_cols, mix_out):
    return (
        lax.all_gather(in_cols.astype(jnp.bfloat16), "fs", axis=0, tiled=True),
        lax.all_gather(mix_out.astype(jnp.bfloat16), "fs", axis=1, tiled=True),
    )


def hidden_units(rows_in, gate_full, up_full, hidden_scales):
    gate = jnp.dot(rows_in, gate_full, preferred_element_type=jnp.float32) * hidden_scales[0]
    upper = jnp.dot(rows_in, up_full, preferred_element_type=jnp.float32) * hidden_scales[1]
    return (jax.nn.silu(gate) * upper).astype(jnp.bfloat16)


def ffn_partial(normed_rows, gate_full, up_full, down_full, hidden_scales, share):

    def term_rows(row_start, row_count):
        hidden = hidden_units(normed_rows, gate_full, up_full, hidden_scales)
        return jnp.dot(hidden, down_full, preferred_element_type=jnp.float32)

    return scatter_rows(term_rows, share)


def per_device(
    tokens,
    norm_gains,
    gate_weight,
    up_weight,
    hidden_scales,
    down_weight,
    down_scale,
    mix_in,
    in_scale,
    pool_map,
    pool_scale,
    mix_out,
    out_scale,
):
    tp_width = lax.axis_size("tp")
    tp_rank = lax.axis_index("tp")
    seq_rows = tokens.shape[0]
    share = seq_rows // tp_width
    local_channels = mix_out.shape[0]
    group_width = pool_map.shape[1]
    needed = max(group_width, local_channels)
    first_channel = tp_rank * local_channels
    in_start = first_channel // group_width * group_width
    in_cols = lax.dynamic_slice_in_dim(mix_in, in_start, needed, 1)
    scale_cols = lax.dynamic_slice_in_dim(in_scale, in_start, needed, 0)
    down_cols, out_cols = (
        lax.all_gather(down_scale, "fs", axis=0, tiled=True),
        lax.all_gather(out_scale, "fs", axis=0, tiled=True),
    )
    gate_bf = gate_weight.astype(jnp.bfloat16)
    up_bf = up_weight.astype(jnp.bfloat16)
    down_bf = down_weight.astype(jnp.bfloat16)
    resid_all = tokens.astype(jnp.float32)
    first = normed(resid_all, norm_gains[0])
    gate_full, up_full, down_full = (
        lax.all_gather(gate_bf, "fs", axis=0, tiled=True),
        lax.all_gather(up_bf, "fs", axis=0, tiled=True),
        lax.all_gather(down_bf, "fs", axis=1, tiled=True),
    )
    ffn_one = ffn_partial(first, gate_full, up_full, down_full, hidden_scales, share)
    own_rows = lax.dynamic_slice_in_dim(resid_all, tp_rank * share, share, 0)
    resid_one = own_rows + 0.5 * (ffn_one * down_cols)
    second = whole_rows(normed(resid_one, norm_gains[1]))
    in_full, out_full = fetch_mixer(in_cols, mix_out)
    pool_in = (jnp.dot(second, in_full, preferred_element_type=jnp.float32) * scale_cols).astype(
        jnp.bfloat16
    )
    channel = in_start + jnp.arange(needed, dtype=jnp.int32)
    window = jnp.left_shift(jnp.int32(2), channel // group_width)
    position = jnp.arange(seq_rows, dtype=jnp.int32)[:, None]
    values = pool_in.astype(jnp.float32)
    summed = jnp.zeros_like(values)
    for offset in range(widest):
        shifted = jnp.pad(values, ((offset, 0), (0, 0)))[:seq_rows]
        summed = summed + jnp.where(offset < window, shifted, 0.0)
    counts = jnp.minimum(position + 1, window).astype(jnp.float32)
    pooled = (summed / counts - values).astype(jnp.bfloat16)
    map_bf = pool_map.astype(jnp.bfloat16)
    if local_channels < group_width:
        group_index = first_channel // group_width
        column_start = first_channel % group_width
        map_cols = lax.dynamic_slice(
            map_bf, (group_index, jnp.int32(0), column_start), (1, group_width, local_channels)
        )[0]
        grouped = jnp.dot(pooled, map_cols, preferred_element_type=jnp.float32)
    else:
        held_groups = local_channels // group_width
        maps_held = lax.dynamic_slice_in_dim(map_bf, first_channel // group_width, held_groups, 0)
        grouped = jnp.einsum(
            "tgc,gcd->tgd",
            pooled.reshape(seq_rows, held_groups, group_width),
            maps_held,
            preferred_element_type=jnp.float32,
        ).reshape(seq_rows, local_channels)
    pool_out = (grouped * pool_scale).astype(jnp.bfloat16)

    def mixer_rows(row_start, row_count):
        return jnp.dot(pool_out, out_full, preferred_element_type=jnp.float32)

    mixed = scatter_rows(mixer_rows, share)
    resid_two = resid_one + mixed * out_cols
    third = whole_rows(normed(resid_two, norm_gains[2]))
    ffn_two = ffn_partial(third, gate_full, up_full, down_full, hidden_scales, share)
    final_rows = (resid_two + 0.5 * (ffn_two * down_cols)).astype(jnp.bfloat16)
    return whole_rows(final_rows)


MESH = pl.DeviceIdType.MESH
PARTS = (1, 1, 4, 4)
FIRST_PART = (0, 1, 2, 6, 10)
TILE = 256
BATCHES = 2
MIXER_AFTER = 2
bf16 = jnp.bfloat16
f32 = jnp.float32


def fits_kernel(mesh):
    return mesh.shape["rep"] == 2 and mesh.shape["fs"] == 4 and mesh.shape["tp"] == 4


def layer_kernel(
    n, tok, gains, gate_hbm, up_hbm, hs, down_hbm, mix_in_hbm, mix_out_hbm, isc, pmap, pool_scale, down_scale, out_scale,
    out, wide_gate, wide_up, wide_down, wide_in, wide_out, sc_in, gu_own, dn_own, gu_buf, dn_buf, wi_all, wo_all, sc_all, ps_all,
    ptok, first, gacc, hidden, stage, rs_a, s_z, rs_z, s_x, rs_x, r1, second, pool, r2, third, stage_2, ra_2, sz_2, rz_2, sx_2, rx_2,
    z_send, y_send, w_recv, sc_send, sc_recv, tp_send, tp_recv, tk_send, tk_recv, rs_send, rs_recv, rt_send, rt_recv, ag_send, ag_recv, loc,
):
    rep, fs, me = lax.axis_index("rep"), lax.axis_index("fs"), lax.axis_index("tp")
    seq, width = tok.shape
    slab = width // n
    share = seq // 4
    rows_half = seq // 2
    halo = widest
    window = rows_half + halo
    units = hs.shape[1]
    hu = units // 2
    groups, gc = pmap.shape[0], pmap.shape[1]
    core, chip = me % 2, me // 2
    mate = me + 1 - 2 * core
    across = (me + 2) % 4
    diag = (mate + 2) % 4
    peers = {1: mate, 2: across, 3: diag}
    partner = fs + 1 - 2 * (fs % 2)
    far_mid = jnp.where(fs < 2, 2, 1)
    far_end = jnp.where(fs < 2, 3, 0)
    order = (fs, partner, far_mid, far_end)
    middle = (fs == 1) | (fs == 2)
    kind = jnp.where(middle, 1, 0)
    kind_of = (kind, 1 - kind, 1, 0)

    def owner_cols(i):
        return pl.ds(pl.multiple_of(order[i] * slab, slab), slab)

    def cols_of(rank):
        return pl.ds(pl.multiple_of(rank * gc, gc), gc)

    half = slab // 2
    mine_half = pl.ds(pl.multiple_of(rep * half, half), half)
    other_half = pl.ds(pl.multiple_of((1 - rep) * half, half), half)
    loads = [
        pltpu.make_async_copy(mix_in_hbm.at[:, cols_of(me)], wide_in, loc.at[0]),
        pltpu.make_async_copy(mix_out_hbm, wide_out, loc.at[1]),
        pltpu.make_async_copy(gate_hbm.at[mine_half, :], wide_gate.at[mine_half, :], loc.at[2]),
        pltpu.make_async_copy(up_hbm.at[mine_half, :], wide_up.at[mine_half, :], loc.at[3]),
        pltpu.make_async_copy(gate_hbm.at[other_half, :], wide_gate.at[other_half, :], loc.at[4]),
        pltpu.make_async_copy(up_hbm.at[other_half, :], wide_up.at[other_half, :], loc.at[5]),
        pltpu.make_async_copy(down_hbm, wide_down, loc.at[6]),
    ]
    for load in loads:
        load.start()
    barrier = pltpu.get_barrier_semaphore()
    for i in (1, 2, 3):
        pl.semaphore_signal(barrier, inc=1, device_id={"fs": order[i]}, device_id_type=MESH)
    for k in (1, 2, 3):
        pl.semaphore_signal(barrier, inc=1, device_id={"tp": peers[k]}, device_id_type=MESH)
    pl.semaphore_signal(barrier, inc=1, device_id={"rep": 1 - rep}, device_id_type=MESH)

    sc_in[...] = jnp.zeros_like(sc_in)
    sc_in[0:1, :] = down_scale[...]
    sc_in[1:2, :] = out_scale[...]
    ps_all[me] = jnp.broadcast_to(pool_scale[...], ps_all.shape[1:])

    WI, WO, GU, DN = range(4)

    def piece(t, i, at, own_kind=None):
        shard = order[i]
        if t == WI:
            return wi_all.at[shard, pl.ds(pl.multiple_of(at * half, half), half), cols_of(me)]
        if t == WO:
            rows = gc // 2
            return wo_all.at[shard, pl.ds(pl.multiple_of(me * gc + at * rows, rows), rows), :]
        ref = (gu_own if t == GU else dn_own).at[own_kind] if own_kind is not None else (gu_buf if t == GU else dn_buf).at[shard]
        rows = ref.shape[0] // (2 * PARTS[t])
        return ref.at[pl.ds(pl.multiple_of(at * rows, rows), rows), :]

    started = []

    def start_if(cond, copy):
        if cond is None:
            copy.start()
        else:
            @pl.when(cond)
            def _():
                copy.start()
        started.append((cond, copy))

    def wait_sent():
        for cond, copy in started:
            if cond is None:
                copy.wait_send()
            else:
                @pl.when(cond)
                def _():
                    copy.wait_send()
        started.clear()

    def remote(src, dst, s_sem, r_sem, dev, cond=None):
        start_if(cond, pltpu.make_async_remote_copy(
            src_ref=src, dst_ref=dst, send_sem=s_sem, recv_sem=r_sem, device_id=dev, device_id_type=MESH
        ))

    def landed(dst, s_sem, r_sem):
        pltpu.make_async_remote_copy(
            src_ref=dst, dst_ref=dst, send_sem=s_sem, recv_sem=r_sem, device_id={"tp": mate}, device_id_type=MESH
        ).wait_recv()

    def send_own(t, i, u, cond=None):
        at = rep * PARTS[t] + u
        remote(
            piece(t, 0, at, kind_of[i] if t >= GU else None), piece(t, 0, at),
            z_send.at[i - 1, FIRST_PART[t] + u], w_recv.at[fs, 2 * FIRST_PART[t] + at], {"fs": order[i]}, cond,
        )

    def arrived(t, i, at):
        landed(piece(t, i, at), z_send.at[0, 0], w_recv.at[order[i], 2 * FIRST_PART[t] + at])

    def relay(t, i, u):
        at = rep * PARTS[t] + u
        arrived(t, i, at)
        here = piece(t, i, at)
        sem = w_recv.at[order[i], 2 * FIRST_PART[t] + at]
        if t < GU and i > 1:
            remote(here, here, y_send.at[0, i, FIRST_PART[t] + u], sem, {"fs": partner}, middle)
        remote(here, here, y_send.at[1, i, FIRST_PART[t] + u], sem, {"rep": 1 - rep})

    def rest(t, i):
        for u in range(PARTS[t]):
            arrived(t, i, (1 - rep) * PARTS[t] + u)

    loads[0].wait()
    loads[1].wait()
    wi_all[fs, :, cols_of(me)] = wide_in[...].astype(bf16)
    wo_all[fs, pl.ds(pl.multiple_of(me * gc, gc), gc), :] = wide_out[...].astype(bf16)

    def cast_gate_up(start, count, kinds):
        @pl.loop(0, count // 32)
        def _(j):
            rows = pl.ds(pl.multiple_of(start + j * 32, 32), 32)
            for h in kinds:
                cols = pl.ds(h * hu if isinstance(h, int) else pl.multiple_of(h * hu, 128), hu)
                gu_own[h, rows, 0:hu] = wide_gate[rows, cols].astype(bf16)
                gu_own[h, rows, hu:] = wide_up[rows, cols].astype(bf16)

    def my_rows(rank):
        return pl.ds(pl.multiple_of(rank * share, share), share)

    pl.semaphore_wait(barrier, n - 1 + 4)
    remote(tok.at[my_rows(me), :], ptok.at[my_rows(me), :], tk_send.at[0], tk_recv.at[0], {"fs": partner})
    loads[2].wait()
    loads[3].wait()
    for u in range(PARTS[GU]):
        cast_gate_up(rep * half + u * (half // PARTS[GU]), half // PARTS[GU], (0, 1))
        for i in (1, 2, 3):
            send_own(GU, i, u)
        if u == MIXER_AFTER:
            for t in (WI, WO):
                for i in (2, 1):
                    send_own(t, i, 0)

    def spread(t, i, rank):
        return wi_all.at[order[i], :, cols_of(rank)] if t == WI else wo_all.at[order[i], pl.ds(pl.multiple_of(rank * gc, gc), gc), :]

    def share_mixer(i):
        for t in (WI, WO):
            mine = spread(t, i, me)
            remote(mine, mine, tp_send.at[t, i, 1], tp_recv.at[t, i, 1], {"tp": across})
            remote(mine, mine, tp_send.at[t, i, 0], tp_recv.at[t, i, 0], {"tp": mate})

    def pass_mixer(i):
        for t in (WI, WO):
            theirs = spread(t, i, across)
            landed(theirs, tp_send.at[t, i, 1], tp_recv.at[t, i, 1])
            remote(theirs, theirs, tp_send.at[t, i, 2], tp_recv.at[t, i, 2], {"tp": mate})

    def have_mixer(i):
        for t in (WI, WO):
            landed(spread(t, i, mate), tp_send.at[t, i, 0], tp_recv.at[t, i, 0])
            landed(spread(t, i, diag), tp_send.at[t, i, 2], tp_recv.at[t, i, 2])

    share_mixer(0)
    loads[4].wait()
    loads[5].wait()
    cast_gate_up((1 - rep) * half, half, (kind,))
    loads[6].wait()

    @pl.loop(0, hu // 32)
    def _(j):
        rows = pl.ds(pl.multiple_of(j * 32, 32), 32)
        for h in (0, 1):
            dn_own[h, rows, :] = wide_down[pl.ds(pl.multiple_of(h * hu + j * 32, 32), 32), :].astype(bf16)

    for i in (1, 2, 3):
        remote(sc_in, sc_all.at[fs], sc_send.at[i - 1], sc_recv.at[fs], {"fs": order[i]})
    for k in (1, 2, 3):
        remote(ps_all.at[me], ps_all.at[me], tp_send.at[2, 0, k - 1], tp_recv.at[2, 0, k - 1], {"tp": peers[k]})

    def normed_rows(values, gain):
        mean_sq = jnp.mean(values * values, axis=-1, keepdims=True)
        return (values * lax.rsqrt(mean_sq + eps) * gain).astype(bf16)

    stage[:, :, 0:halo, :] = jnp.zeros((n, 2, halo, slab), bf16)

    def norm_first(source, top):
        @pl.loop(0, seq // 32)
        def _(j):
            rows = pl.ds(pl.multiple_of(j * 32, 32), 32)
            first[pl.ds(pl.multiple_of(top + j * 32, 32), 32), :] = normed_rows(source[rows, :].astype(f32), gains[0:1, :])

    def dot(a, b):
        return jnp.dot(a, b, preferred_element_type=f32)

    def held_gu(i):
        return gu_own.at[kind] if i == 0 else gu_buf.at[order[i]]

    def held_dn(i):
        return dn_own.at[kind] if i == 0 else dn_buf.at[order[i]]

    def gate_up(i, fresh):
        weights = held_gu(i)
        cols = owner_cols(i)

        @pl.loop(0, 2 * hu // TILE)
        def _(j):
            at = pl.ds(pl.multiple_of(j * TILE, TILE), TILE)
            term = dot(first[:, cols], weights[:, at])
            if fresh:
                gacc[:, at] = term
            else:
                gacc[:, at] += term

    def activate(rows):
        @pl.loop(0, hu // 128)
        def _(j):
            at = pl.ds(pl.multiple_of(j * 128, 128), 128)
            up_at = pl.ds(pl.multiple_of(hu + j * 128, 128), 128)
            sc_at = pl.ds(pl.multiple_of(kind * hu + j * 128, 128), 128)
            gate = gacc[rows, at] * hs[0:1, sc_at]
            upper = gacc[rows, up_at] * hs[1:2, sc_at]
            hidden[rows, at] = (gate / (1.0 + jnp.exp(-gate)) * upper).astype(bf16)

    def down(i, side):
        weights = held_dn(i)

        @pl.loop(0, slab // TILE)
        def _(j):
            at = pl.ds(pl.multiple_of(j * TILE, TILE), TILE)
            stage[i, side, halo:, at] = dot(hidden[side * seq:(side + 1) * seq, :], weights[:, at]).astype(bf16)

    norm_first(tok, 0)
    own_rows = my_rows(me)
    landed(ptok.at[own_rows, :], tk_send.at[0], tk_recv.at[0])
    for k in (2, 3, 1):
        remote(ptok.at[own_rows, :], ptok.at[own_rows, :], tk_send.at[k], tk_recv.at[k], {"tp": peers[k]})
    def relay_mixer(i):
        for t in (WI, WO):
            relay(t, i, 0)

    def rest_mixer(i):
        rest(WI, i)
        rest(WO, i)
        share_mixer(i)

    for u in range(PARTS[GU]):
        for i in (1, 2, 3):
            relay(GU, i, u)
        if u == 1:
            for k in (1, 2, 3):
                landed(ptok.at[my_rows(peers[k]), :], tk_send.at[k], tk_recv.at[k])
            for i in (1, 2, 3):
                for v in range(PARTS[DN]):
                    send_own(DN, i, v, middle if i == 3 else None)
            norm_first(ptok, seq)
        if u == 2:
            relay_mixer(1)
            gate_up(0, True)
    relay_mixer(2)
    relay_mixer(3)
    rest_mixer(1)
    rest(GU, 1)
    gate_up(1, False)
    pass_mixer(0)
    rest(GU, 2)
    gate_up(2, False)
    rest_mixer(2)
    rest_mixer(3)
    rest(GU, 3)
    gate_up(3, False)
    activate(slice(None))

    for i in (1, 2, 3):
        landed(sc_all.at[order[i]], sc_send.at[0], sc_recv.at[order[i]])

    def scales(i):
        return sc_in if i == 0 else sc_all.at[order[i]]

    def half_of(c):
        return pl.ds(pl.multiple_of(c * rows_half, rows_half), rows_half)

    before = pl.ds(pl.multiple_of((core * rows_half + seq - halo) % seq, halo), halo)
    batch = rows_half // BATCHES
    whole = ((0, window),)
    split = tuple((b * batch + (halo if b else 0), batch + (0 if b else halo)) for b in range(BATCHES))

    def parts(i):
        return split if i == n - 1 else whole

    def window_of(c, part):
        return pl.ds(pl.multiple_of(c * rows_half + part[0], halo), part[1])

    def cut_a(i):
        for side in (1, 0):
            down(i, side)
            for p, part in enumerate(parts(i)):
                remote(
                    stage.at[i, side, window_of(1 - core, part), :], rs_a.at[i, side, pl.ds(*part), :],
                    rs_send.at[p, i, side], rs_recv.at[p, i, side], {"tp": mate},
                )

    def cross_a(i):
        for p, part in enumerate(parts(i)):
            rows = pl.ds(*part)
            landed(rs_a.at[i, 1, rows, :], rs_send.at[p, i, 1], rs_recv.at[p, i, 1])
            s_z[i, rows, :] = (stage[i, 1, window_of(core, part), :].astype(f32) + rs_a[i, 1, rows, :].astype(f32)).astype(bf16)
            remote(
                s_z.at[i, rows, :], rs_z.at[order[i], rows, :], rs_send.at[p, i, 2], rs_recv.at[p, order[i], 2], {"fs": partner}
            )

    def fold_a(i, p=0):
        part = parts(i)[p]
        rows = pl.ds(*part)
        landed(rs_a.at[i, 0, rows, :], rs_send.at[p, i, 0], rs_recv.at[p, i, 0])
        landed(rs_z.at[order[i], rows, :], rs_send.at[p, i, 2], rs_recv.at[p, order[i], 2])
        total = stage[i, 0, window_of(core, part), :].astype(f32) + rs_a[i, 0, rows, :].astype(f32)
        s_x[i, rows, :] = (total + rs_z[order[i], rows, :].astype(f32)).astype(bf16)
        remote(s_x.at[i, rows, :], rs_x.at[i, rows, :], rs_send.at[p, i, 3], rs_recv.at[p, i, 3], {"tp": across})

    def gather_a(i, p=0):
        part = parts(i)[p]
        top, count = part
        rows = pl.ds(*part)
        landed(rs_x.at[i, rows, :], rs_send.at[p, i, 3], rs_recv.at[p, i, 3])
        total = 0.5 * ((s_x[i, rows, :].astype(f32) + rs_x[i, rows, :].astype(f32)) * scales(i)[0:1, :])
        cols = owner_cols(i)
        if top == 0:
            r1[0:halo, cols] = total[0:halo] + jnp.where(core > 0, tok[before, cols].astype(f32), 0.0)
            total, top, count = total[halo:], halo, count - halo
        held = pl.ds(pl.multiple_of(core * rows_half + top - halo, halo), count)
        r1[top:top + count, cols] = total + tok[held, cols].astype(f32)

    cut_a(0)
    for u in range(PARTS[DN]):
        relay(DN, 1, u)
    cross_a(0)
    for u in range(PARTS[DN]):
        send_own(DN, 3, u, ~middle)
    for u in range(PARTS[DN]):
        relay(DN, 2, u)
    pass_mixer(1)
    rest(DN, 1)
    cut_a(1)
    cross_a(1)
    fold_a(0)
    for u in range(PARTS[DN]):
        relay(DN, 3, u)
    rest(DN, 2)
    cut_a(2)
    pass_mixer(2)
    cross_a(2)
    fold_a(1)
    rest(DN, 3)
    cut_a(3)
    pass_mixer(3)
    cross_a(3)
    gather_a(0)
    fold_a(2)
    gather_a(1)
    for k in (1, 2, 3):
        landed(ps_all.at[peers[k]], tp_send.at[2, 0, k - 1], tp_recv.at[2, 0, k - 1])
    for i in range(n):
        have_mixer(i)
    gather_a(2)

    def mixer(b):
        low = b * batch
        taken = slice(low, low + batch + halo)
        second[...] = normed_rows(r1[taken, :], gains[1:2, :])
        total = dot(second[:, owner_cols(0)], wi_all[order[0]])
        for i in range(1, n):
            total = total + dot(second[:, owner_cols(i)], wi_all[order[i]])
        values = (total * isc[...]).astype(bf16).astype(f32)
        sums = values
        position = lax.broadcasted_iota(jnp.int32, (batch, gc), 0) + (core * rows_half + low)
        for g in range(groups):
            span = 2 ** (g + 1)
            sums = sums + pltpu.roll(sums, span // 2, 0)
            at = slice(g * gc, (g + 1) * gc)
            counts = jnp.minimum(position + 1, span).astype(f32)
            pooled = (sums[halo:, 0:gc] / counts - values[halo:, at]).astype(bf16)
            pool[:, at] = (dot(pooled, pmap[g].astype(bf16)) * ps_all[g, 0:1, :]).astype(bf16)
            sums = sums[:, gc:]
        rows = slice(low, low + batch)
        for i in range(n):
            cols = owner_cols(i)
            r2[rows, cols] = r1[low + halo:low + halo + batch, cols] + dot(pool[...], wo_all[order[i]]) * scales(i)[1:2, :]
        third[lot(b, 0, core), :] = normed_rows(r2[rows, :], gains[2:3, :])

    def lot(b, side, c):
        return pl.ds(pl.multiple_of(((b * 2 + side) * 2 + c) * batch, batch), batch)

    def piece_of(b, side, c, x):
        return pl.ds(pl.multiple_of(((b * 2 + side) * 2 + c) * batch + x * (batch // 2), batch // 2), batch // 2)

    def both(b, side):
        return slice((b * 2 + side) * 2 * batch, (b * 2 + side + 1) * 2 * batch)

    def send_third(b):
        remote(third.at[piece_of(b, 0, core, chip), :], third.at[piece_of(b, 1, core, chip), :], ag_send.at[b, 1], ag_recv.at[b, 1], {"fs": partner})
        mine = third.at[lot(b, 0, core), :]
        remote(mine, mine, ag_send.at[b, 0], ag_recv.at[b, 0], {"tp": mate})

    def have_own(b):
        landed(third.at[lot(b, 0, 1 - core), :], ag_send.at[b, 0], ag_recv.at[b, 0])

    def forward_third(b):
        here = third.at[piece_of(b, 1, core, chip), :]
        landed(here, ag_send.at[b, 1], ag_recv.at[b, 1])
        remote(here, here, ag_send.at[b, 2], ag_recv.at[b, 2], {"tp": across})
        remote(here, here, ag_send.at[b, 3], ag_recv.at[b, 3], {"tp": mate})

    def pass_third(b):
        there = third.at[piece_of(b, 1, core, 1 - chip), :]
        landed(there, ag_send.at[b, 2], ag_recv.at[b, 2])
        remote(there, there, ag_send.at[b, 4], ag_recv.at[b, 4], {"tp": mate})

    def have_partner(b):
        landed(third.at[piece_of(b, 1, 1 - core, chip), :], ag_send.at[b, 3], ag_recv.at[b, 3])
        landed(third.at[piece_of(b, 1, 1 - core, 1 - chip), :], ag_send.at[b, 4], ag_recv.at[b, 4])

    def hidden_rows(b, side):
        rows = both(b, side)

        @pl.loop(0, 2 * hu // TILE)
        def _(j):
            at = pl.ds(pl.multiple_of(j * TILE, TILE), TILE)
            acc = dot(third[rows, owner_cols(0)], held_gu(0)[:, at])
            for i in range(1, n):
                acc = acc + dot(third[rows, owner_cols(i)], held_gu(i)[:, at])
            gacc[rows, at] = acc

        activate(rows)

    def down_send(i, b, side):
        rows = both(b, side)
        stage_2[i, rows, :] = dot(hidden[rows, :], held_dn(i)[...]).astype(bf16)
        remote(stage_2.at[i, lot(b, side, 1 - core), :], ra_2.at[i, b, side], rt_send.at[i, b, side], rt_recv.at[i, b, side], {"tp": mate})

    def cross_b(i, b):
        landed(ra_2.at[i, b, 1], rt_send.at[i, b, 1], rt_recv.at[i, b, 1])
        sz_2[i, b] = (stage_2[i, lot(b, 1, core), :].astype(f32) + ra_2[i, b, 1].astype(f32)).astype(bf16)
        remote(sz_2.at[i, b], rz_2.at[order[i], b], rt_send.at[i, b, 2], rt_recv.at[order[i], b, 2], {"fs": partner})

    def fold_b(i, b):
        landed(ra_2.at[i, b, 0], rt_send.at[i, b, 0], rt_recv.at[i, b, 0])
        landed(rz_2.at[order[i], b], rt_send.at[i, b, 2], rt_recv.at[order[i], b, 2])
        total = stage_2[i, lot(b, 0, core), :].astype(f32) + ra_2[i, b, 0].astype(f32) + rz_2[order[i], b].astype(f32)
        sx_2[i, b] = total.astype(bf16)
        remote(sx_2.at[i, b], rx_2.at[i, b], rt_send.at[i, b, 3], rt_recv.at[i, b, 3], {"tp": across})

    def out_rows(b, c):
        return pl.ds(pl.multiple_of(c * rows_half + b * batch, batch), batch)

    def final_b(i, b):
        landed(rx_2.at[i, b], rt_send.at[i, b, 3], rt_recv.at[i, b, 3])
        total = 0.5 * ((sx_2[i, b].astype(f32) + rx_2[i, b].astype(f32)) * scales(i)[0:1, :])
        cols = owner_cols(i)
        out[out_rows(b, core), cols] = (r2[b * batch:(b + 1) * batch, cols] + total).astype(bf16)
        done = out.at[out_rows(b, core), cols]
        remote(done, done, rt_send.at[i, b, 4], rt_recv.at[i, b, 4], {"tp": mate})

    for b in range(BATCHES):
        if b == 0:
            for q in range(BATCHES):
                fold_a(n - 1, q)
        gather_a(n - 1, b)
        mixer(b)
        send_third(b)
    have_own(0)
    hidden_rows(0, 0)
    forward_third(0)
    have_own(1)
    hidden_rows(1, 0)
    forward_third(1)
    pass_third(0)
    for i in range(n):
        down_send(i, 0, 0)
    have_partner(0)
    hidden_rows(0, 1)
    for i in range(n):
        down_send(i, 0, 1)
    pass_third(1)
    for i in range(n):
        cross_b(i, 0)
    have_partner(1)
    hidden_rows(1, 1)
    fold_b(0, 0)
    for i in range(n):
        down_send(i, 1, 1)
    fold_b(1, 0)
    for i in range(n):
        cross_b(i, 1)
    fold_b(2, 0)
    final_b(0, 0)
    for i in range(n):
        down_send(i, 1, 0)
    fold_b(3, 0)
    final_b(1, 0)
    final_b(2, 0)
    fold_b(0, 1)
    final_b(n - 1, 0)
    for i in range(n):
        if i + 1 < n:
            fold_b(i + 1, 1)
        final_b(i, 1)
    for b in range(BATCHES):
        for i in range(n):
            landed(out.at[out_rows(b, 1 - core), owner_cols(i)], rt_send.at[i, b, 4], rt_recv.at[i, b, 4])
    wait_sent()


def fused_layer(
    tokens, norm_gains, gate_weight, up_weight, hidden_scales, down_weight, down_scale, mix_in, in_scale,
    pool_map, pool_scale, mix_out, out_scale,
):
    n = lax.axis_size("fs")
    seq, width = tokens.shape
    slab, units = gate_weight.shape
    hu = units // 2
    groups, gc, _ = pool_map.shape
    rows_half = seq // 2
    window = rows_half + widest
    batch = rows_half // BATCHES
    vmem = pl.BlockSpec(memory_space=pltpu.VMEM)
    dma = pltpu.SemaphoreType.DMA
    hbm = pl.BlockSpec(memory_space=pl.ANY)
    args = (
        (tokens, vmem), (norm_gains, vmem), (gate_weight, hbm), (up_weight, hbm), (hidden_scales, vmem),
        (down_weight, hbm), (mix_in, hbm), (mix_out, hbm), (in_scale[None], vmem), (pool_map, vmem),
        (pool_scale[None], vmem), (down_scale[None], vmem), (out_scale[None], vmem),
    )
    return pl.pallas_call(
        functools.partial(layer_kernel, n),
        out_shape=pltpu.VMEM((seq, width), bf16),
        in_specs=[spec for _, spec in args],
        out_specs=vmem,
        scratch_shapes=[
            pltpu.VMEM((slab, units), f32),
            pltpu.VMEM((slab, units), f32),
            pltpu.VMEM((units, slab), f32),
            pltpu.VMEM((slab, gc), f32),
            pltpu.VMEM((gc, slab), f32),
            pltpu.VMEM((8, slab), f32),
            pltpu.VMEM((2, slab, 2 * hu), bf16),
            pltpu.VMEM((2, hu, slab), bf16),
            pltpu.VMEM((n, slab, 2 * hu), bf16),
            pltpu.VMEM((n, hu, slab), bf16),
            pltpu.VMEM((n, slab, groups * gc), bf16),
            pltpu.VMEM((n, groups * gc, slab), bf16),
            pltpu.VMEM((n, 8, slab), f32),
            pltpu.VMEM((4, 8, gc), f32),
            pltpu.VMEM((seq, width), bf16),
            pltpu.VMEM((2 * seq, width), bf16),
            pltpu.VMEM((2 * seq, 2 * hu), f32),
            pltpu.VMEM((2 * seq, hu), bf16),
            pltpu.VMEM((n, 2, seq + widest, slab), bf16),
            pltpu.VMEM((n, 2, window, slab), bf16),
            pltpu.VMEM((n, window, slab), bf16),
            pltpu.VMEM((n, window, slab), bf16),
            pltpu.VMEM((n, window, slab), bf16),
            pltpu.VMEM((n, window, slab), bf16),
            pltpu.VMEM((window, width), f32),
            pltpu.VMEM((batch + widest, width), bf16),
            pltpu.VMEM((batch, groups * gc), bf16),
            pltpu.VMEM((rows_half, width), f32),
            pltpu.VMEM((2 * seq, width), bf16),
            pltpu.VMEM((n, 2 * seq, slab), bf16),
            pltpu.VMEM((n, BATCHES, 2, batch, slab), bf16),
            pltpu.VMEM((n, BATCHES, batch, slab), bf16),
            pltpu.VMEM((n, BATCHES, batch, slab), bf16),
            pltpu.VMEM((n, BATCHES, batch, slab), bf16),
            pltpu.VMEM((n, BATCHES, batch, slab), bf16),
            dma((n - 1, FIRST_PART[-1])), dma((2, n, FIRST_PART[-1])), dma((n, 2 * FIRST_PART[-1])),
            dma((n - 1,)), dma((n,)),
            dma((3, n, 3)), dma((3, n, 3)),
            dma((4,)), dma((4,)),
            dma((BATCHES, n, 4)), dma((BATCHES, n, 4)),
            dma((n, BATCHES, 5)), dma((n, BATCHES, 5)),
            dma((BATCHES, 5)), dma((BATCHES, 5)),
            dma((7,)),
        ],
        compiler_params=pltpu.CompilerParams(
            collective_id=0, has_side_effects=True, vmem_limit_bytes=62 * 1024 * 1024
        ),
    )(*[value for value, _ in args])


def solution(mesh):
    body = fused_layer if fits_kernel(mesh) else per_device
    return jax.shard_map(
        body,
        mesh=mesh,
        in_specs=(
            P(("rep", "fs"), None),
            P(),
            P("fs", "tp"),
            P("fs", "tp"),
            P(None, "tp"),
            P("tp", "fs"),
            P("fs"),
            P("fs", None),
            P(),
            P(),
            P("tp"),
            P("tp", "fs"),
            P("fs"),
        ),
        out_specs=P(("rep", "fs"), None),
        check_vma=False,
    )
```

```python
import functools

import jax
import jax.numpy as jnp
from jax import lax
from jax.experimental import pallas as pl
from jax.experimental.pallas import tpu as pltpu
from jax.sharding import PartitionSpec as P

eps = 1e-06
widest = 16


def normed(values, gain):
    mean_sq = jnp.mean(values * values, axis=-1, keepdims=True)
    return (values * lax.rsqrt(mean_sq + eps) * gain).astype(jnp.bfloat16)


def scatter_rows(term_fn, share):
    return lax.psum_scatter(
        term_fn(jnp.int32(0), lax.axis_size("tp") * share).astype(jnp.bfloat16),
        "tp",
        scatter_dimension=0,
        tiled=True,
    ).astype(jnp.float32)


def whole_rows(values):
    return lax.all_gather(values, "tp", axis=0, tiled=True)


def fetch_mixer(in_cols, mix_out):
    return (
        lax.all_gather(in_cols.astype(jnp.bfloat16), "fs", axis=0, tiled=True),
        lax.all_gather(mix_out.astype(jnp.bfloat16), "fs", axis=1, tiled=True),
    )


def hidden_units(rows_in, gate_full, up_full, hidden_scales):
    gate = jnp.dot(rows_in, gate_full, preferred_element_type=jnp.float32) * hidden_scales[0]
    upper = jnp.dot(rows_in, up_full, preferred_element_type=jnp.float32) * hidden_scales[1]
    return (jax.nn.silu(gate) * upper).astype(jnp.bfloat16)


def ffn_partial(normed_rows, gate_full, up_full, down_full, hidden_scales, share):

    def term_rows(row_start, row_count):
        hidden = hidden_units(normed_rows, gate_full, up_full, hidden_scales)
        return jnp.dot(hidden, down_full, preferred_element_type=jnp.float32)

    return scatter_rows(term_rows, share)


def per_device(
    tokens,
    norm_gains,
    gate_weight,
    up_weight,
    hidden_scales,
    down_weight,
    down_scale,
    mix_in,
    in_scale,
    pool_map,
    pool_scale,
    mix_out,
    out_scale,
):
    tp_width = lax.axis_size("tp")
    tp_rank = lax.axis_index("tp")
    seq_rows = tokens.shape[0]
    share = seq_rows // tp_width
    local_channels = mix_out.shape[0]
    group_width = pool_map.shape[1]
    needed = max(group_width, local_channels)
    first_channel = tp_rank * local_channels
    in_start = first_channel // group_width * group_width
    in_cols = lax.dynamic_slice_in_dim(mix_in, in_start, needed, 1)
    scale_cols = lax.dynamic_slice_in_dim(in_scale, in_start, needed, 0)
    down_cols, out_cols = (
        lax.all_gather(down_scale, "fs", axis=0, tiled=True),
        lax.all_gather(out_scale, "fs", axis=0, tiled=True),
    )
    gate_bf = gate_weight.astype(jnp.bfloat16)
    up_bf = up_weight.astype(jnp.bfloat16)
    down_bf = down_weight.astype(jnp.bfloat16)
    resid_all = tokens.astype(jnp.float32)
    first = normed(resid_all, norm_gains[0])
    gate_full, up_full, down_full = (
        lax.all_gather(gate_bf, "fs", axis=0, tiled=True),
        lax.all_gather(up_bf, "fs", axis=0, tiled=True),
        lax.all_gather(down_bf, "fs", axis=1, tiled=True),
    )
    ffn_one = ffn_partial(first, gate_full, up_full, down_full, hidden_scales, share)
    own_rows = lax.dynamic_slice_in_dim(resid_all, tp_rank * share, share, 0)
    resid_one = own_rows + 0.5 * (ffn_one * down_cols)
    second = whole_rows(normed(resid_one, norm_gains[1]))
    in_full, out_full = fetch_mixer(in_cols, mix_out)
    pool_in = (jnp.dot(second, in_full, preferred_element_type=jnp.float32) * scale_cols).astype(
        jnp.bfloat16
    )
    channel = in_start + jnp.arange(needed, dtype=jnp.int32)
    window = jnp.left_shift(jnp.int32(2), channel // group_width)
    position = jnp.arange(seq_rows, dtype=jnp.int32)[:, None]
    values = pool_in.astype(jnp.float32)
    summed = jnp.zeros_like(values)
    for offset in range(widest):
        shifted = jnp.pad(values, ((offset, 0), (0, 0)))[:seq_rows]
        summed = summed + jnp.where(offset < window, shifted, 0.0)
    counts = jnp.minimum(position + 1, window).astype(jnp.float32)
    pooled = (summed / counts - values).astype(jnp.bfloat16)
    map_bf = pool_map.astype(jnp.bfloat16)
    if local_channels < group_width:
        group_index = first_channel // group_width
        column_start = first_channel % group_width
        map_cols = lax.dynamic_slice(
            map_bf, (group_index, jnp.int32(0), column_start), (1, group_width, local_channels)
        )[0]
        grouped = jnp.dot(pooled, map_cols, preferred_element_type=jnp.float32)
    else:
        held_groups = local_channels // group_width
        maps_held = lax.dynamic_slice_in_dim(map_bf, first_channel // group_width, held_groups, 0)
        grouped = jnp.einsum(
            "tgc,gcd->tgd",
            pooled.reshape(seq_rows, held_groups, group_width),
            maps_held,
            preferred_element_type=jnp.float32,
        ).reshape(seq_rows, local_channels)
    pool_out = (grouped * pool_scale).astype(jnp.bfloat16)

    def mixer_rows(row_start, row_count):
        return jnp.dot(pool_out, out_full, preferred_element_type=jnp.float32)

    mixed = scatter_rows(mixer_rows, share)
    resid_two = resid_one + mixed * out_cols
    third = whole_rows(normed(resid_two, norm_gains[2]))
    ffn_two = ffn_partial(third, gate_full, up_full, down_full, hidden_scales, share)
    final_rows = (resid_two + 0.5 * (ffn_two * down_cols)).astype(jnp.bfloat16)
    return whole_rows(final_rows)


MESH = pl.DeviceIdType.MESH
PARTS = (1, 1, 4, 2)
FIRST_PART = (0, 1, 2, 6, 8)
TILE = 256
BATCHES = 2
MIXER_AFTER = 2
bf16 = jnp.bfloat16
f32 = jnp.float32


def fits_kernel(mesh):
    return mesh.shape["rep"] == 2 and mesh.shape["fs"] == 4 and mesh.shape["tp"] == 4


def layer_kernel(
    n, tok_hbm, gains, gate_hbm, up_hbm, hs, down_hbm, mix_in_hbm, mix_out_hbm, isc, pmap_hbm, pool_scale, down_scale, out_scale,
    out, tok, pmap, wide_gate, wide_up, wide_down, wide_in, wide_out, sc_in, gu_own, dn_own, gu_buf, dn_buf, wi_all, wo_all, sc_all, ps_all,
    ptok, first, gacc, hidden, stage, rs_a, s_z, rs_z, s_x, rs_x, r1, second, pool, r2, third, stage_2, ra_2, sz_2, rz_2, sx_2, rx_2,
    z_send, y_send, w_recv, sc_send, sc_recv, tp_send, tp_recv, tk_send, tk_recv, rs_send, rs_recv, rt_send, rt_recv, ag_send, ag_recv, loc,
):
    rep, fs, me = lax.axis_index("rep"), lax.axis_index("fs"), lax.axis_index("tp")
    seq, width = tok.shape
    slab = width // n
    share = seq // 4
    rows_half = seq // 2
    halo = widest
    window = rows_half + halo
    units = hs.shape[1]
    hu = units // 2
    groups, gc = pmap.shape[0], pmap.shape[1]
    core, chip = me % 2, me // 2
    mate = me + 1 - 2 * core
    across = (me + 2) % 4
    diag = (mate + 2) % 4
    peers = {1: mate, 2: across, 3: diag}
    partner = fs + 1 - 2 * (fs % 2)
    far_mid = jnp.where(fs < 2, 2, 1)
    far_end = jnp.where(fs < 2, 3, 0)
    order = (fs, partner, far_mid, far_end)
    middle = (fs == 1) | (fs == 2)
    kind = jnp.where(middle, 1, 0)
    kind_of = (kind, 1 - kind, 1, 0)

    def owner_cols(i):
        return pl.ds(pl.multiple_of(order[i] * slab, slab), slab)

    def cols_of(rank):
        return pl.ds(pl.multiple_of(rank * gc, gc), gc)

    half = slab // 2
    mine_half = pl.ds(pl.multiple_of(rep * half, half), half)
    other_half = pl.ds(pl.multiple_of((1 - rep) * half, half), half)
    loads = [
        pltpu.make_async_copy(mix_in_hbm.at[:, cols_of(me)], wide_in, loc.at[0]),
        pltpu.make_async_copy(mix_out_hbm, wide_out, loc.at[1]),
        pltpu.make_async_copy(gate_hbm.at[mine_half, :], wide_gate.at[mine_half, :], loc.at[2]),
        pltpu.make_async_copy(up_hbm.at[mine_half, :], wide_up.at[mine_half, :], loc.at[3]),
        pltpu.make_async_copy(gate_hbm.at[other_half, :], wide_gate.at[other_half, :], loc.at[4]),
        pltpu.make_async_copy(up_hbm.at[other_half, :], wide_up.at[other_half, :], loc.at[5]),
        pltpu.make_async_copy(tok_hbm, tok, loc.at[7]),
        pltpu.make_async_copy(down_hbm, wide_down, loc.at[6]),
        pltpu.make_async_copy(pmap_hbm, pmap, loc.at[8]),
    ]
    for load in loads:
        load.start()
    barrier = pltpu.get_barrier_semaphore()
    for i in (1, 2, 3):
        pl.semaphore_signal(barrier, inc=1, device_id={"fs": order[i]}, device_id_type=MESH)
    for k in (1, 2, 3):
        pl.semaphore_signal(barrier, inc=1, device_id={"tp": peers[k]}, device_id_type=MESH)
    pl.semaphore_signal(barrier, inc=1, device_id={"rep": 1 - rep}, device_id_type=MESH)

    sc_in[...] = jnp.zeros_like(sc_in)
    sc_in[0:1, :] = down_scale[...]
    sc_in[1:2, :] = out_scale[...]
    ps_all[me] = jnp.broadcast_to(pool_scale[...], ps_all.shape[1:])

    WI, WO, GU, DN = range(4)

    def piece(t, i, at, own_kind=None):
        shard = order[i]
        if t == WI:
            return wi_all.at[shard, pl.ds(pl.multiple_of(at * half, half), half), cols_of(me)]
        if t == WO:
            rows = gc // 2
            return wo_all.at[shard, pl.ds(pl.multiple_of(me * gc + at * rows, rows), rows), :]
        ref = (gu_own if t == GU else dn_own).at[own_kind] if own_kind is not None else (gu_buf if t == GU else dn_buf).at[shard]
        rows = ref.shape[0] // (2 * PARTS[t])
        return ref.at[pl.ds(pl.multiple_of(at * rows, rows), rows), :]

    started = []

    def start_if(cond, copy):
        if cond is None:
            copy.start()
        else:
            @pl.when(cond)
            def _():
                copy.start()
        started.append((cond, copy))

    def wait_sent():
        for cond, copy in started:
            if cond is None:
                copy.wait_send()
            else:
                @pl.when(cond)
                def _():
                    copy.wait_send()
        started.clear()

    def remote(src, dst, s_sem, r_sem, dev, cond=None):
        start_if(cond, pltpu.make_async_remote_copy(
            src_ref=src, dst_ref=dst, send_sem=s_sem, recv_sem=r_sem, device_id=dev, device_id_type=MESH
        ))

    def landed(dst, s_sem, r_sem):
        pltpu.make_async_remote_copy(
            src_ref=dst, dst_ref=dst, send_sem=s_sem, recv_sem=r_sem, device_id={"tp": mate}, device_id_type=MESH
        ).wait_recv()

    def send_own(t, i, u, cond=None):
        at = rep * PARTS[t] + u
        remote(
            piece(t, 0, at, kind_of[i] if t >= GU else None), piece(t, 0, at),
            z_send.at[i - 1, FIRST_PART[t] + u], w_recv.at[fs, 2 * FIRST_PART[t] + at], {"fs": order[i]}, cond,
        )

    def arrived(t, i, at):
        landed(piece(t, i, at), z_send.at[0, 0], w_recv.at[order[i], 2 * FIRST_PART[t] + at])

    def relay(t, i, u):
        at = rep * PARTS[t] + u
        arrived(t, i, at)
        here = piece(t, i, at)
        sem = w_recv.at[order[i], 2 * FIRST_PART[t] + at]
        if t < GU and i > 1:
            remote(here, here, y_send.at[0, i, FIRST_PART[t] + u], sem, {"fs": partner}, middle)
        remote(here, here, y_send.at[1, i, FIRST_PART[t] + u], sem, {"rep": 1 - rep})

    def rest(t, i):
        for u in range(PARTS[t]):
            arrived(t, i, (1 - rep) * PARTS[t] + u)

    loads[0].wait()
    loads[1].wait()
    wi_all[fs, :, cols_of(me)] = wide_in[...].astype(bf16)
    wo_all[fs, pl.ds(pl.multiple_of(me * gc, gc), gc), :] = wide_out[...].astype(bf16)

    def cast_gate_up(start, count, kinds):
        @pl.loop(0, count // 32)
        def _(j):
            rows = pl.ds(pl.multiple_of(start + j * 32, 32), 32)
            for h in kinds:
                cols = pl.ds(h * hu if isinstance(h, int) else pl.multiple_of(h * hu, 128), hu)
                gu_own[h, rows, 0:hu] = wide_gate[rows, cols].astype(bf16)
                gu_own[h, rows, hu:] = wide_up[rows, cols].astype(bf16)

    def my_rows(rank):
        return pl.ds(pl.multiple_of(rank * share, share), share)

    pl.semaphore_wait(barrier, n - 1 + 4)
    loads[6].wait()
    remote(tok.at[my_rows(me), :], ptok.at[my_rows(me), :], tk_send.at[0], tk_recv.at[0], {"fs": partner})
    loads[2].wait()
    loads[3].wait()
    for u in range(PARTS[GU]):
        cast_gate_up(rep * half + u * (half // PARTS[GU]), half // PARTS[GU], (0, 1))
        for i in (1, 2, 3):
            send_own(GU, i, u)
        if u == MIXER_AFTER:
            for t in (WI, WO):
                for i in (2, 1):
                    send_own(t, i, 0)

    def spread(t, i, rank):
        return wi_all.at[order[i], :, cols_of(rank)] if t == WI else wo_all.at[order[i], pl.ds(pl.multiple_of(rank * gc, gc), gc), :]

    def share_mixer(i):
        for t in (WI, WO):
            mine = spread(t, i, me)
            remote(mine, mine, tp_send.at[t, i, 1], tp_recv.at[t, i, 1], {"tp": across})
            remote(mine, mine, tp_send.at[t, i, 0], tp_recv.at[t, i, 0], {"tp": mate})

    def pass_mixer(i):
        for t in (WI, WO):
            theirs = spread(t, i, across)
            landed(theirs, tp_send.at[t, i, 1], tp_recv.at[t, i, 1])
            remote(theirs, theirs, tp_send.at[t, i, 2], tp_recv.at[t, i, 2], {"tp": mate})

    def have_mixer(i):
        for t in (WI, WO):
            landed(spread(t, i, mate), tp_send.at[t, i, 0], tp_recv.at[t, i, 0])
            landed(spread(t, i, diag), tp_send.at[t, i, 2], tp_recv.at[t, i, 2])

    share_mixer(0)
    loads[4].wait()
    loads[5].wait()
    cast_gate_up((1 - rep) * half, half, (kind,))
    loads[7].wait()
    loads[8].wait()

    @pl.loop(0, hu // 32)
    def _(j):
        rows = pl.ds(pl.multiple_of(j * 32, 32), 32)
        for h in (0, 1):
            dn_own[h, rows, :] = wide_down[pl.ds(pl.multiple_of(h * hu + j * 32, 32), 32), :].astype(bf16)

    for i in (1, 2, 3):
        remote(sc_in, sc_all.at[fs], sc_send.at[i - 1], sc_recv.at[fs], {"fs": order[i]})
    for k in (1, 2, 3):
        remote(ps_all.at[me], ps_all.at[me], tp_send.at[2, 0, k - 1], tp_recv.at[2, 0, k - 1], {"tp": peers[k]})

    def normed_rows(values, gain):
        mean_sq = jnp.mean(values * values, axis=-1, keepdims=True)
        return (values * lax.rsqrt(mean_sq + eps) * gain).astype(bf16)

    stage[:, :, 0:halo, :] = jnp.zeros((n, 2, halo, slab), bf16)

    def norm_first(source, top):
        @pl.loop(0, seq // 32)
        def _(j):
            rows = pl.ds(pl.multiple_of(j * 32, 32), 32)
            first[pl.ds(pl.multiple_of(top + j * 32, 32), 32), :] = normed_rows(source[rows, :].astype(f32), gains[0:1, :])

    def dot(a, b):
        return jnp.dot(a, b, preferred_element_type=f32)

    def held_gu(i):
        return gu_own.at[kind] if i == 0 else gu_buf.at[order[i]]

    def held_dn(i):
        return dn_own.at[kind] if i == 0 else dn_buf.at[order[i]]

    def gate_up(i, fresh):
        weights = held_gu(i)
        cols = owner_cols(i)

        @pl.loop(0, 2 * hu // TILE)
        def _(j):
            at = pl.ds(pl.multiple_of(j * TILE, TILE), TILE)
            term = dot(first[:, cols], weights[:, at])
            if fresh:
                gacc[:, at] = term
            else:
                gacc[:, at] += term

    def activate(rows):
        @pl.loop(0, hu // 128)
        def _(j):
            at = pl.ds(pl.multiple_of(j * 128, 128), 128)
            up_at = pl.ds(pl.multiple_of(hu + j * 128, 128), 128)
            sc_at = pl.ds(pl.multiple_of(kind * hu + j * 128, 128), 128)
            gate = gacc[rows, at] * hs[0:1, sc_at]
            upper = gacc[rows, up_at] * hs[1:2, sc_at]
            hidden[rows, at] = (gate / (1.0 + jnp.exp(-gate)) * upper).astype(bf16)

    def down(i, side):
        weights = held_dn(i)

        @pl.loop(0, slab // TILE)
        def _(j):
            at = pl.ds(pl.multiple_of(j * TILE, TILE), TILE)
            stage[i, side, halo:, at] = dot(hidden[side * seq:(side + 1) * seq, :], weights[:, at]).astype(bf16)

    norm_first(tok, 0)
    own_rows = my_rows(me)
    landed(ptok.at[own_rows, :], tk_send.at[0], tk_recv.at[0])
    for k in (2, 3, 1):
        remote(ptok.at[own_rows, :], ptok.at[own_rows, :], tk_send.at[k], tk_recv.at[k], {"tp": peers[k]})
    def relay_mixer(i):
        for t in (WI, WO):
            relay(t, i, 0)

    def rest_mixer(i):
        rest(WI, i)
        rest(WO, i)
        share_mixer(i)

    for u in range(PARTS[GU]):
        for i in (1, 2, 3):
            relay(GU, i, u)
        if u == 1:
            for k in (1, 2, 3):
                landed(ptok.at[my_rows(peers[k]), :], tk_send.at[k], tk_recv.at[k])
            for i in (1, 2, 3):
                for v in range(PARTS[DN]):
                    send_own(DN, i, v, middle if i == 3 else None)
            norm_first(ptok, seq)
        if u == 2:
            relay_mixer(1)
            gate_up(0, True)
    relay_mixer(2)
    relay_mixer(3)
    rest_mixer(1)
    rest(GU, 1)
    gate_up(1, False)
    pass_mixer(0)
    rest(GU, 2)
    gate_up(2, False)
    rest_mixer(2)
    rest_mixer(3)
    rest(GU, 3)
    gate_up(3, False)
    activate(slice(None))

    for i in (1, 2, 3):
        landed(sc_all.at[order[i]], sc_send.at[0], sc_recv.at[order[i]])

    def scales(i):
        return sc_in if i == 0 else sc_all.at[order[i]]

    def half_of(c):
        return pl.ds(pl.multiple_of(c * rows_half, rows_half), rows_half)

    before = pl.ds(pl.multiple_of((core * rows_half + seq - halo) % seq, halo), halo)
    batch = rows_half // BATCHES
    whole = ((0, window),)
    split = tuple((b * batch + (halo if b else 0), batch + (0 if b else halo)) for b in range(BATCHES))

    def parts(i):
        return split if i == n - 1 else whole

    def window_of(c, part):
        return pl.ds(pl.multiple_of(c * rows_half + part[0], halo), part[1])

    def cut_a(i):
        for side in (1, 0):
            down(i, side)
            for p, part in enumerate(parts(i)):
                remote(
                    stage.at[i, side, window_of(1 - core, part), :], rs_a.at[i, side, pl.ds(*part), :],
                    rs_send.at[p, i, side], rs_recv.at[p, i, side], {"tp": mate},
                )

    def cross_a(i):
        for p, part in enumerate(parts(i)):
            rows = pl.ds(*part)
            landed(rs_a.at[i, 1, rows, :], rs_send.at[p, i, 1], rs_recv.at[p, i, 1])
            s_z[i, rows, :] = (stage[i, 1, window_of(core, part), :].astype(f32) + rs_a[i, 1, rows, :].astype(f32)).astype(bf16)
            remote(
                s_z.at[i, rows, :], rs_z.at[order[i], rows, :], rs_send.at[p, i, 2], rs_recv.at[p, order[i], 2], {"fs": partner}
            )

    def fold_a(i, p=0):
        part = parts(i)[p]
        rows = pl.ds(*part)
        landed(rs_a.at[i, 0, rows, :], rs_send.at[p, i, 0], rs_recv.at[p, i, 0])
        landed(rs_z.at[order[i], rows, :], rs_send.at[p, i, 2], rs_recv.at[p, order[i], 2])
        total = stage[i, 0, window_of(core, part), :].astype(f32) + rs_a[i, 0, rows, :].astype(f32)
        s_x[i, rows, :] = (total + rs_z[order[i], rows, :].astype(f32)).astype(bf16)
        remote(s_x.at[i, rows, :], rs_x.at[i, rows, :], rs_send.at[p, i, 3], rs_recv.at[p, i, 3], {"tp": across})

    def gather_a(i, p=0):
        part = parts(i)[p]
        top, count = part
        rows = pl.ds(*part)
        landed(rs_x.at[i, rows, :], rs_send.at[p, i, 3], rs_recv.at[p, i, 3])
        total = 0.5 * ((s_x[i, rows, :].astype(f32) + rs_x[i, rows, :].astype(f32)) * scales(i)[0:1, :])
        cols = owner_cols(i)
        if top == 0:
            r1[0:halo, cols] = total[0:halo] + jnp.where(core > 0, tok[before, cols].astype(f32), 0.0)
            total, top, count = total[halo:], halo, count - halo
        held = pl.ds(pl.multiple_of(core * rows_half + top - halo, halo), count)
        r1[top:top + count, cols] = total + tok[held, cols].astype(f32)

    cut_a(0)
    for u in range(PARTS[DN]):
        relay(DN, 1, u)
    cross_a(0)
    for u in range(PARTS[DN]):
        send_own(DN, 3, u, ~middle)
    for u in range(PARTS[DN]):
        relay(DN, 2, u)
    pass_mixer(1)
    rest(DN, 1)
    cut_a(1)
    cross_a(1)
    fold_a(0)
    for u in range(PARTS[DN]):
        relay(DN, 3, u)
    rest(DN, 2)
    cut_a(2)
    pass_mixer(2)
    cross_a(2)
    fold_a(1)
    rest(DN, 3)
    cut_a(3)
    pass_mixer(3)
    cross_a(3)
    gather_a(0)
    fold_a(2)
    gather_a(1)
    def mixer(b):
        low = b * batch
        taken = slice(low, low + batch + halo)
        second[...] = normed_rows(r1[taken, :], gains[1:2, :])
        total = dot(second[:, owner_cols(0)], wi_all[order[0]])
        for i in range(1, n):
            total = total + dot(second[:, owner_cols(i)], wi_all[order[i]])
        values = (total * isc[...]).astype(bf16).astype(f32)
        sums = values
        position = lax.broadcasted_iota(jnp.int32, (batch, gc), 0) + (core * rows_half + low)
        for g in range(groups):
            span = 2 ** (g + 1)
            sums = sums + pltpu.roll(sums, span // 2, 0)
            at = slice(g * gc, (g + 1) * gc)
            counts = jnp.minimum(position + 1, span).astype(f32)
            pooled = (sums[halo:, 0:gc] / counts - values[halo:, at]).astype(bf16)
            pool[:, at] = (dot(pooled, pmap[g].astype(bf16)) * ps_all[g, 0:1, :]).astype(bf16)
            sums = sums[:, gc:]
        rows = slice(low, low + batch)
        for i in range(n):
            cols = owner_cols(i)
            r2[rows, cols] = r1[low + halo:low + halo + batch, cols] + dot(pool[...], wo_all[order[i]]) * scales(i)[1:2, :]
        third[lot(b, 0, core), :] = normed_rows(r2[rows, :], gains[2:3, :])

    def lot(b, side, c):
        return pl.ds(pl.multiple_of(((b * 2 + side) * 2 + c) * batch, batch), batch)

    def piece_of(b, side, c, x):
        return pl.ds(pl.multiple_of(((b * 2 + side) * 2 + c) * batch + x * (batch // 2), batch // 2), batch // 2)

    def both(b, side):
        return slice((b * 2 + side) * 2 * batch, (b * 2 + side + 1) * 2 * batch)

    def send_third(b):
        remote(third.at[piece_of(b, 0, core, chip), :], third.at[piece_of(b, 1, core, chip), :], ag_send.at[b, 1], ag_recv.at[b, 1], {"fs": partner})
        mine = third.at[lot(b, 0, core), :]
        remote(mine, mine, ag_send.at[b, 0], ag_recv.at[b, 0], {"tp": mate})

    def have_own(b):
        landed(third.at[lot(b, 0, 1 - core), :], ag_send.at[b, 0], ag_recv.at[b, 0])

    def forward_third(b):
        here = third.at[piece_of(b, 1, core, chip), :]
        landed(here, ag_send.at[b, 1], ag_recv.at[b, 1])
        remote(here, here, ag_send.at[b, 2], ag_recv.at[b, 2], {"tp": across})
        remote(here, here, ag_send.at[b, 3], ag_recv.at[b, 3], {"tp": mate})

    def pass_third(b):
        there = third.at[piece_of(b, 1, core, 1 - chip), :]
        landed(there, ag_send.at[b, 2], ag_recv.at[b, 2])
        remote(there, there, ag_send.at[b, 4], ag_recv.at[b, 4], {"tp": mate})

    def have_partner(b):
        landed(third.at[piece_of(b, 1, 1 - core, chip), :], ag_send.at[b, 3], ag_recv.at[b, 3])
        landed(third.at[piece_of(b, 1, 1 - core, 1 - chip), :], ag_send.at[b, 4], ag_recv.at[b, 4])

    def hidden_rows(b, side):
        rows = both(b, side)

        @pl.loop(0, 2 * hu // TILE)
        def _(j):
            at = pl.ds(pl.multiple_of(j * TILE, TILE), TILE)
            acc = dot(third[rows, owner_cols(0)], held_gu(0)[:, at])
            for i in range(1, n):
                acc = acc + dot(third[rows, owner_cols(i)], held_gu(i)[:, at])
            gacc[rows, at] = acc

        activate(rows)

    def down_send(i, b, side):
        rows = both(b, side)
        stage_2[i, rows, :] = dot(hidden[rows, :], held_dn(i)[...]).astype(bf16)
        remote(stage_2.at[i, lot(b, side, 1 - core), :], ra_2.at[i, b, side], rt_send.at[i, b, side], rt_recv.at[i, b, side], {"tp": mate})

    def cross_b(i, b):
        landed(ra_2.at[i, b, 1], rt_send.at[i, b, 1], rt_recv.at[i, b, 1])
        sz_2[i, b] = (stage_2[i, lot(b, 1, core), :].astype(f32) + ra_2[i, b, 1].astype(f32)).astype(bf16)
        remote(sz_2.at[i, b], rz_2.at[order[i], b], rt_send.at[i, b, 2], rt_recv.at[order[i], b, 2], {"fs": partner})

    def fold_b(i, b):
        landed(ra_2.at[i, b, 0], rt_send.at[i, b, 0], rt_recv.at[i, b, 0])
        landed(rz_2.at[order[i], b], rt_send.at[i, b, 2], rt_recv.at[order[i], b, 2])
        total = stage_2[i, lot(b, 0, core), :].astype(f32) + ra_2[i, b, 0].astype(f32) + rz_2[order[i], b].astype(f32)
        sx_2[i, b] = total.astype(bf16)
        remote(sx_2.at[i, b], rx_2.at[i, b], rt_send.at[i, b, 3], rt_recv.at[i, b, 3], {"tp": across})

    def out_rows(b, c):
        return pl.ds(pl.multiple_of(c * rows_half + b * batch, batch), batch)

    def final_b(i, b):
        landed(rx_2.at[i, b], rt_send.at[i, b, 3], rt_recv.at[i, b, 3])
        total = 0.5 * ((sx_2[i, b].astype(f32) + rx_2[i, b].astype(f32)) * scales(i)[0:1, :])
        cols = owner_cols(i)
        out[out_rows(b, core), cols] = (r2[b * batch:(b + 1) * batch, cols] + total).astype(bf16)
        done = out.at[out_rows(b, core), cols]
        remote(done, done, rt_send.at[i, b, 4], rt_recv.at[i, b, 4], {"tp": mate})

    for b in range(BATCHES):
        if b == 0:
            for q in range(BATCHES):
                fold_a(n - 1, q)
            gather_a(2)
            for k in (1, 2, 3):
                landed(ps_all.at[peers[k]], tp_send.at[2, 0, k - 1], tp_recv.at[2, 0, k - 1])
            for i in range(n):
                have_mixer(i)
        gather_a(n - 1, b)
        mixer(b)
        send_third(b)
    have_own(0)
    hidden_rows(0, 0)
    forward_third(0)
    have_own(1)
    hidden_rows(1, 0)
    forward_third(1)
    pass_third(0)
    for i in range(n):
        down_send(i, 0, 0)
    have_partner(0)
    hidden_rows(0, 1)
    for i in range(n):
        down_send(i, 0, 1)
    pass_third(1)
    for i in range(n):
        cross_b(i, 0)
    have_partner(1)
    hidden_rows(1, 1)
    fold_b(0, 0)
    for i in range(n):
        down_send(i, 1, 1)
    fold_b(1, 0)
    for i in range(n):
        cross_b(i, 1)
    fold_b(2, 0)
    final_b(0, 0)
    for i in range(n):
        down_send(i, 1, 0)
    fold_b(3, 0)
    final_b(1, 0)
    final_b(2, 0)
    fold_b(0, 1)
    final_b(n - 1, 0)
    for i in range(n):
        if i + 1 < n:
            fold_b(i + 1, 1)
        final_b(i, 1)
    for b in range(BATCHES):
        for i in range(n):
            landed(out.at[out_rows(b, 1 - core), owner_cols(i)], rt_send.at[i, b, 4], rt_recv.at[i, b, 4])
    wait_sent()


def fused_layer(
    tokens, norm_gains, gate_weight, up_weight, hidden_scales, down_weight, down_scale, mix_in, in_scale,
    pool_map, pool_scale, mix_out, out_scale,
):
    n = lax.axis_size("fs")
    seq, width = tokens.shape
    slab, units = gate_weight.shape
    hu = units // 2
    groups, gc, _ = pool_map.shape
    rows_half = seq // 2
    window = rows_half + widest
    batch = rows_half // BATCHES
    vmem = pl.BlockSpec(memory_space=pltpu.VMEM)
    dma = pltpu.SemaphoreType.DMA
    hbm = pl.BlockSpec(memory_space=pl.ANY)
    args = (
        (tokens, hbm), (norm_gains, vmem), (gate_weight, hbm), (up_weight, hbm), (hidden_scales, vmem),
        (down_weight, hbm), (mix_in, hbm), (mix_out, hbm), (in_scale[None], vmem), (pool_map, hbm),
        (pool_scale[None], vmem), (down_scale[None], vmem), (out_scale[None], vmem),
    )
    return pl.pallas_call(
        functools.partial(layer_kernel, n),
        out_shape=pltpu.VMEM((seq, width), bf16),
        in_specs=[spec for _, spec in args],
        out_specs=vmem,
        scratch_shapes=[
            pltpu.VMEM((seq, width), bf16),
            pltpu.VMEM(pool_map.shape, f32),
            pltpu.VMEM((slab, units), f32),
            pltpu.VMEM((slab, units), f32),
            pltpu.VMEM((units, slab), f32),
            pltpu.VMEM((slab, gc), f32),
            pltpu.VMEM((gc, slab), f32),
            pltpu.VMEM((8, slab), f32),
            pltpu.VMEM((2, slab, 2 * hu), bf16),
            pltpu.VMEM((2, hu, slab), bf16),
            pltpu.VMEM((n, slab, 2 * hu), bf16),
            pltpu.VMEM((n, hu, slab), bf16),
            pltpu.VMEM((n, slab, groups * gc), bf16),
            pltpu.VMEM((n, groups * gc, slab), bf16),
            pltpu.VMEM((n, 8, slab), f32),
            pltpu.VMEM((4, 8, gc), f32),
            pltpu.VMEM((seq, width), bf16),
            pltpu.VMEM((2 * seq, width), bf16),
            pltpu.VMEM((2 * seq, 2 * hu), f32),
            pltpu.VMEM((2 * seq, hu), bf16),
            pltpu.VMEM((n, 2, seq + widest, slab), bf16),
            pltpu.VMEM((n, 2, window, slab), bf16),
            pltpu.VMEM((n, window, slab), bf16),
            pltpu.VMEM((n, window, slab), bf16),
            pltpu.VMEM((n, window, slab), bf16),
            pltpu.VMEM((n, window, slab), bf16),
            pltpu.VMEM((window, width), f32),
            pltpu.VMEM((batch + widest, width), bf16),
            pltpu.VMEM((batch, groups * gc), bf16),
            pltpu.VMEM((rows_half, width), f32),
            pltpu.VMEM((2 * seq, width), bf16),
            pltpu.VMEM((n, 2 * seq, slab), bf16),
            pltpu.VMEM((n, BATCHES, 2, batch, slab), bf16),
            pltpu.VMEM((n, BATCHES, batch, slab), bf16),
            pltpu.VMEM((n, BATCHES, batch, slab), bf16),
            pltpu.VMEM((n, BATCHES, batch, slab), bf16),
            pltpu.VMEM((n, BATCHES, batch, slab), bf16),
            dma((n - 1, FIRST_PART[-1])), dma((2, n, FIRST_PART[-1])), dma((n, 2 * FIRST_PART[-1])),
            dma((n - 1,)), dma((n,)),
            dma((3, n, 3)), dma((3, n, 3)),
            dma((4,)), dma((4,)),
            dma((BATCHES, n, 4)), dma((BATCHES, n, 4)),
            dma((n, BATCHES, 5)), dma((n, BATCHES, 5)),
            dma((BATCHES, 5)), dma((BATCHES, 5)),
            dma((9,)),
        ],
        compiler_params=pltpu.CompilerParams(
            collective_id=0, has_side_effects=True, vmem_limit_bytes=62 * 1024 * 1024
        ),
    )(*[value for value, _ in args])


def solution(mesh):
    body = fused_layer if fits_kernel(mesh) else per_device
    return jax.shard_map(
        body,
        mesh=mesh,
        in_specs=(
            P(("rep", "fs"), None),
            P(),
            P("fs", "tp"),
            P("fs", "tp"),
            P(None, "tp"),
            P("tp", "fs"),
            P("fs"),
            P("fs", None),
            P(),
            P(),
            P("tp"),
            P("tp", "fs"),
            P("fs"),
        ),
        out_specs=P(("rep", "fs"), None),
        check_vma=False,
    )
```
